32 devices in a mesh: grp: 2 (over y), sp: 4 (over z), tp: 4 (over x, core).
Axes of the slice: x: 2, y: 2, z: 4, core: 2. Of those that a mesh axis runs over, the one named last changes fastest.
Arguments:
- prompt: bfloat16 [8, 6144, 2048], P('grp', 'sp'), parts along dimension 0, may hold values from -6 to 6
- w_key: bfloat16 [2048, 2048], P('sp', 'tp'), may hold values from -0.125 to 0.125
- w_value: bfloat16 [2048, 2048], P('sp', 'tp'), may hold values from -0.125 to 0.125
- query_new: bfloat16 [8, 2048], P('grp', 'tp'), parts along dimension 0, may hold values from -150 to 150
- key_new: bfloat16 [8, 2048], P('grp', 'tp'), parts along dimension 0, may hold values from -15 to 15
- value_new: bfloat16 [8, 2048], P('grp', 'tp'), parts along dimension 0, may hold values from -6 to 6
- mix_lambda: float32 [16], P('tp'), may hold values from 0.3 to 0.8
- head_gain: float32 [128], replicated, may hold values from 0.1 to 1.9
Outputs:
- key_cache: bfloat16 [8, 4, 1536, 2048], P(('grp', 'sp'), None, None, 'tp'), parts along dimension 0
- value_cache: bfloat16 [8, 4, 1536, 2048], P(('grp', 'sp'), None, None, 'tp'), parts along dimension 0
- first_read: bfloat16 [8, 2048], P('grp', 'tp'), parts along dimension 0
The draws below stay inside these ranges and needn't reach their ends.
There are 2 independent parts, one for each index of `grp`. The reference program is written for one: setup_inputs(seed, part) draws one part's arguments, and reference() takes and returns one part's arrays. A program takes and returns all parts, laid end to end along the dimension named above; an argument that names none is the same for every part. Nothing has to cross between parts.
All inputs are finite; a program needn't handle non-finite values.
Results may differ from the reference program's by a relative error of at most 0.0065.
The reference program's roundings to bfloat16 on the way (of `keys`, `values` and `mixed`) count: a program that leaves them out, or rounds other values in their place, can miss the bound.
Values may be sent and summed in bfloat16 or wider, within the bound.
A program may use at most 128 MiB of HBM per device.

```python
import jax
import jax.numpy as jnp
from jax import lax

D = 2048
HEADS = 16
HALF = 64
VDIM = 128
SEQS = 4
LEN = 6144
N_SP = 4


def draw_query_new(key, part):
    base = jax.random.normal(key, (SEQS, HEADS, 2 * HALF), jnp.float32) * 1.75
    return jnp.clip(base, -10.0, 10.0).reshape(SEQS, HEADS * 2 * HALF).astype(jnp.bfloat16)


def levels(own_key, extent, pieces, least, high):
    def one(position, blocks):
        steps = jax.random.uniform(jax.random.fold_in(jax.random.fold_in(own_key, 6), position), (blocks,), jnp.float32, least / len(pieces), high / len(pieces))
        return jnp.repeat(jnp.exp(steps), extent[position] // blocks).reshape((-1,) + (1,) * (len(extent) - position - 1))

    gain = one(*pieces[0])
    for cut in pieces[1:]:
        gain = gain * one(*cut)
    return gain


def scatter_about(stream_key, shape, width, limit, cuts=(), kind=jnp.bfloat16):
    array = jax.random.normal(stream_key, shape, jnp.float32) * width
    if len(cuts) > 0:
        array = levels(stream_key, shape, cuts, -0.22, 0.18) * array
    return jnp.clip(array, min=-limit, max=limit).astype(kind)


def setup_inputs(seed: int = 0, part: int = 0) -> dict:
    seeds = jax.random.split(jax.random.key(seed), 9)
    own_keys = jax.random.split(jax.random.fold_in(seeds[8], part), 9)
    return {
        "prompt": scatter_about(own_keys[0], (SEQS, LEN, D), 1.0, 6.0, ((1, 4),)),
        "w_key": scatter_about(seeds[1], (D, HEADS * 2 * HALF), D ** -0.5, 0.125, ((0, 4), (1, 4))),
        "w_value": scatter_about(seeds[2], (D, HEADS * VDIM), D ** -0.5, 0.125, ((0, 4), (1, 4))),
        "query_new": draw_query_new(jax.random.fold_in(jax.random.fold_in(seeds[8], part), 71), part),
        "key_new": scatter_about(own_keys[4], (SEQS, HEADS * 2 * HALF), 2.5, 15.0, ((1, 4),)),
        "value_new": scatter_about(own_keys[5], (SEQS, HEADS * VDIM), 1.0, 6.0, ((1, 4),)),
        "mix_lambda": jnp.clip(0.3 + 0.5 * jax.random.uniform(seeds[6], (HEADS,), jnp.float32) ** levels(seeds[6], (HEADS,), ((0, 4),), -0.2, 0.2), 0.3, 0.8),
        "head_gain": jnp.clip(1.0 + 0.18 * jax.random.normal(seeds[7], (VDIM,), jnp.float32), 0.1, 1.9),
    }


def reference(prompt, w_key, w_value, query_new, key_new, value_new, mix_lambda, head_gain):
    rows = prompt.reshape(SEQS * LEN, D)
    keys = jnp.dot(rows, w_key, preferred_element_type=jnp.float32).astype(jnp.bfloat16)
    values = jnp.dot(rows, w_value, preferred_element_type=jnp.float32).astype(jnp.bfloat16)
    keys = keys.reshape(SEQS, LEN, HEADS * 2 * HALF)
    values = values.reshape(SEQS, LEN, HEADS * VDIM)
    scale = HALF ** (-0.5)

    def one_prompt(args):
        query, fresh_key, fresh_value, cached_keys, cached_values = args
        q_parts = query.astype(jnp.float32).reshape(HEADS, 2, HALF)
        k_parts = cached_keys.astype(jnp.float32).reshape(LEN, HEADS, 2, HALF)
        scores = jnp.einsum('hmc,lhmc->hml', q_parts, k_parts) * scale
        fresh = lax.optimization_barrier(jnp.sum(q_parts * fresh_key.astype(jnp.float32).reshape(HEADS, 2, HALF), axis=-1)) * scale
        top = jnp.maximum(lax.optimization_barrier(jnp.max(scores, axis=-1)), fresh)
        weights = jnp.exp(scores - top[..., None])
        own = jnp.exp(fresh - top)
        total = lax.optimization_barrier(jnp.sum(weights, axis=-1)) + own
        probs = weights / total[..., None]
        own_prob = own / total
        mixed = (probs[:, 0] - mix_lambda[:, None] * probs[:, 1]).astype(jnp.bfloat16)
        own_mixed = (own_prob[:, 0] - mix_lambda * own_prob[:, 1]).astype(jnp.bfloat16)
        value_parts = cached_values.astype(jnp.float32).reshape(LEN, HEADS, VDIM)
        reads = jnp.einsum('hl,lhv->hv', mixed.astype(jnp.float32), value_parts)
        reads = reads + own_mixed.astype(jnp.float32)[:, None] * fresh_value.astype(jnp.float32).reshape(HEADS, VDIM)
        mean = lax.optimization_barrier(jnp.mean(reads * reads, axis=-1, keepdims=True))
        normed = reads * lax.rsqrt(mean + 1e-06) * head_gain
        return normed.reshape(HEADS * VDIM).astype(jnp.bfloat16)
    first_read = lax.map(one_prompt, (query_new, key_new, value_new, keys, values))
    group = N_SP // SEQS
    sub = LEN // N_SP // group
    key_cache = keys.reshape(SEQS, N_SP, group, sub, HEADS * 2 * HALF).transpose(0, 2, 1, 3, 4)
    key_cache = key_cache.reshape(SEQS * group, N_SP, sub, HEADS * 2 * HALF)
    value_cache = values.reshape(SEQS, N_SP, group, sub, HEADS * VDIM).transpose(0, 2, 1, 3, 4)
    value_cache = value_cache.reshape(SEQS * group, N_SP, sub, HEADS * VDIM)
    return (key_cache, value_cache, first_read)
```

```python
import functools

import jax
import jax.numpy as jnp
from jax import lax
from jax.experimental import pallas as pl
from jax.experimental.pallas import tpu as pltpu
from jax.sharding import PartitionSpec as P

HALF = 64
VDIM = 128
MESH = pl.DeviceIdType.MESH
BIG = 256
FILL = 128
SMALL = 64


def combined_all(part, axis, combine):
    gathered = jax.tree.map(lambda a: lax.all_gather(a, axis), part)

    def take(source):
        return jax.tree.map(lambda a: lax.dynamic_index_in_dim(a, source, 0, False), gathered)

    return lax.fori_loop(
        1, lax.axis_size(axis), lambda source, state: combine(state, take(source)), take(0)
    )


def project(rows, w_key, w_value):
    keys = jnp.dot(
        rows, lax.all_gather(w_key, "sp", axis=0, tiled=True), preferred_element_type=jnp.float32
    )
    values = jnp.dot(
        rows, lax.all_gather(w_value, "sp", axis=0, tiled=True), preferred_element_type=jnp.float32
    )
    return (keys.astype(jnp.bfloat16), values.astype(jnp.bfloat16))


def score_maps(query, keys):
    count, span = (keys.shape[0], keys.shape[1])
    heads = query.shape[1] // (2 * HALF)
    q_parts = query.reshape(count, heads, 2, HALF)
    k_parts = keys.reshape(count, span, heads, 2, HALF)
    return jnp.einsum(
        "shmc,slhmc->shml", q_parts, k_parts, preferred_element_type=jnp.float32
    ) * HALF ** (-0.5)


def own_scores(query, fresh_key):
    count = query.shape[0]
    heads = query.shape[1] // (2 * HALF)
    q_parts = query.astype(jnp.float32).reshape(count, heads, 2, HALF)
    k_parts = fresh_key.astype(jnp.float32).reshape(count, heads, 2, HALF)
    return jnp.sum(q_parts * k_parts, axis=-1) * HALF ** (-0.5)


def finish(reads, head_gain):
    mean = jnp.mean(reads * reads, axis=-1, keepdims=True)
    normed = reads * lax.rsqrt(mean + 1e-06) * head_gain
    return normed.reshape(reads.shape[0], -1).astype(jnp.bfloat16)


def join_totals(first, second):
    top = jnp.maximum(first[0], second[0])
    return (top, first[1] * jnp.exp(first[0] - top) + second[1] * jnp.exp(second[0] - top))


def placed(part_rows, prompts, first, fill):
    base = jnp.full((prompts,) + part_rows.shape[1:], fill, jnp.float32)
    return lax.dynamic_update_slice_in_dim(base, part_rows, first, 0)


def cache_read(query_new, key_new, value_new, keys, values, mix_lambda, head_gain, first):
    count, span = (keys.shape[0], keys.shape[1])
    prompts = query_new.shape[0]
    heads = mix_lambda.shape[0]
    query = lax.dynamic_slice_in_dim(query_new, first, count, 0)
    scores = score_maps(query, keys)
    fresh_all = own_scores(query_new, key_new)
    fresh = lax.dynamic_slice_in_dim(fresh_all, first, count, 0)
    local_top = jnp.maximum(jnp.max(scores, axis=-1), fresh)
    local_total = jnp.sum(jnp.exp(scores - local_top[..., None]), axis=-1)
    top_all, cache_total = combined_all(
        (placed(local_top, prompts, first, -1e30), placed(local_total, prompts, first, 0.0)),
        "sp",
        join_totals,
    )
    own = jnp.exp(fresh_all - top_all)
    total_all = cache_total + own
    top = lax.dynamic_slice_in_dim(top_all, first, count, 0)
    total = lax.dynamic_slice_in_dim(total_all, first, count, 0)
    probs = jnp.exp(scores - top[..., None]) / total[..., None]
    mixed = (probs[:, :, 0] - mix_lambda[None, :, None] * probs[:, :, 1]).astype(jnp.bfloat16)
    value_parts = values.reshape(count, span, heads, VDIM)
    partial_value = jnp.einsum(
        "shl,slhv->shv", mixed, value_parts, preferred_element_type=jnp.float32
    )
    reads = lax.psum(placed(partial_value, prompts, first, 0.0), "sp")
    own_prob = own / total_all
    own_mixed = (own_prob[:, :, 0] - mix_lambda[None, :] * own_prob[:, :, 1]).astype(jnp.bfloat16)
    reads = reads + own_mixed.astype(jnp.float32)[..., None] * value_new.astype(
        jnp.float32
    ).reshape(prompts, heads, VDIM)
    return finish(reads, head_gain)


def block_read(
    query_new, key_new, value_new, key_cache, value_cache, mix_lambda, head_gain, spread
):
    blocks, sub = (key_cache.shape[1], key_cache.shape[2])
    first = lax.axis_index("sp") // spread
    keys = key_cache.reshape(1, blocks * sub, -1)
    values = value_cache.reshape(1, blocks * sub, -1)
    return cache_read(query_new, key_new, value_new, keys, values, mix_lambda, head_gain, first)


def body(prompt, w_key, w_value, query_new, key_new, value_new, mix_lambda, head_gain):
    count, piece, width = prompt.shape
    spread = lax.axis_size("sp") // count
    sub = piece // spread
    keys, values = project(prompt.reshape(count * piece, width), w_key, w_value)
    key_blocks = keys.reshape(count * spread, 1, sub, -1)
    value_blocks = values.reshape(count * spread, 1, sub, -1)
    key_cache, value_cache = (
        lax.all_to_all(key_blocks, "sp", split_axis=0, concat_axis=1, tiled=True),
        lax.all_to_all(value_blocks, "sp", split_axis=0, concat_axis=1, tiled=True),
    )
    first_read = block_read(
        query_new, key_new, value_new, key_cache, value_cache, mix_lambda, head_gain, spread
    )
    return (key_cache, value_cache, first_read)


def critical(n, spot):
    return n // 2 - 1 if spot >= n // 2 else n // 2


def crosses(n, src, dst):
    return critical(n, dst) == src


def right_plan(n, blocks, src):
    far_first = list(range(n - 1, src, -1))
    if src == n // 2 - 1:
        early = [(dst, "fill", 0) for dst in far_first]
        late = [(dst, "big", j) for j in range(blocks - 1) for dst in far_first]
        late += [(dst, "small", j) for j in range(2) for dst in far_first]
        return early, late
    if src < n // 2 - 1:
        near = [dst for dst in far_first if dst < n // 2]
        rest = [dst for dst in far_first if dst >= n // 2]
        return (
            [(dst, "big", j) for j in range(blocks) for dst in near],
            [(dst, "big", j) for j in range(blocks) for dst in rest],
        )
    early = [(dst, "big", 0) for dst in far_first]
    return early, [(dst, "big", j) for j in range(1, blocks) for dst in far_first]


def left_plan(n, blocks, src):
    early, late = right_plan(n, blocks, n - 1 - src)
    flip = lambda items: [(n - 1 - dst, kind, j) for dst, kind, j in items]
    return flip(early), flip(late)


def arrivals(n, blocks, spot):
    if spot >= n // 2:
        first, rest = arrivals(n, blocks, n - 1 - spot)
        flip = lambda items: [(kind, n - 1 - src, j) for kind, src, j in items]
        return flip(first), flip(rest)
    crit = n // 2
    same = sorted((s for s in range(n // 2) if s != spot), key=lambda s: abs(s - spot))
    other = [s for s in range(n // 2 + 1, n)]
    by_distance = sorted((s for s in range(n) if s != spot), key=lambda s: abs(s - spot))
    ahead = 3 if spot == n // 2 - 1 else 1
    near_w = [s for s in by_distance if abs(s - spot) == 1]
    far_w = [s for s in by_distance if abs(s - spot) > 1]
    first = [("w", s, 0) for s in near_w] + [("fill", crit, 0)]
    first += [("big", same[0], j) for j in range(ahead)]
    first += [("w", s, 0) for s in far_w]
    near = [("big", s, j) for j in range(blocks) for s in same][ahead:]
    through = [("big", s, j) for j in range(blocks) for s in other]
    last = [("big", crit, j) for j in range(blocks - 1)]
    if spot == n // 2 - 1:
        rest = near[:2] + last[:1] + near[2:] + through + last[1:]
    else:
        mixed = []
        for a in range(max(len(near), len(through))):
            mixed += near[a:a + 1] + through[a:a + 1]
        rest = last[:2] + mixed + last[2:]
    return first, rest


def gather_kernel(
    plan, prompt, w_key, w_value, query, key_new, value_new, lam, gain,
    keys, values, read,
    rows_in, weights, scores, q_low, own, slots,
    q_in, k_in, v_in, lam_in, gain_in,
    z_send, z_recv, x_send, x_recv, d_send, d_recv, e_send, e_recv,
    wr_send, wr_recv, wl_send, wl_recv, wy_send, wy_recv, s_send, s_recv, local,
):
    n, piece = plan
    blocks = piece // BIG
    slots_per = blocks + 2
    me = lax.axis_index("sp")
    tp = lax.axis_index("tp")
    grp = lax.axis_index("grp")
    across = lax.rem(tp + 2, 4)
    sibling = tp + 1 - 2 * lax.rem(tp, 2)
    far = lax.rem(sibling + 2, 4)
    depth, cols = w_key.shape
    heads = cols // VDIM
    half = depth // 2
    mats = (w_key, w_value)

    def by_spot(values_):
        pick = values_[0]
        for spot in range(1, n):
            pick = jnp.where(me == spot, values_[spot], pick)
        return pick

    crit = by_spot([critical(n, spot) for spot in range(n)])

    def span(kind, j):
        if kind == "big":
            return j * BIG, BIG, j
        if kind == "fill":
            return piece - BIG, FILL, blocks - 1
        return piece - 2 * SMALL + j * SMALL, SMALL, blocks + j

    def part(kind, j, q):
        start, size, _ = span(kind, j)
        quarter = size // 4
        return pl.ds(pl.multiple_of(start + q * quarter, quarter), quarter)

    barrier = pltpu.get_barrier_semaphore()
    for step in range(1, n):
        pl.semaphore_signal(
            barrier, inc=1, device_id={"sp": lax.rem(me + step, n)}, device_id_type=MESH
        )
    pl.semaphore_signal(barrier, inc=1, device_id={"tp": across}, device_id_type=MESH)
    pl.semaphore_signal(barrier, inc=1, device_id={"tp": sibling}, device_id_type=MESH)
    pl.semaphore_signal(barrier, inc=1, device_id={"grp": 1 - grp}, device_id_type=MESH)
    pl.semaphore_wait(barrier, n + 2)

    def w_slot(src, m, g):
        return weights.at[pl.ds(pl.multiple_of(src * depth + g * half, half), half),
                          pl.ds(m * cols, cols)]

    def w_hop(src, m, to, send, recv, own_):
        origin = mats[m].at[pl.ds(pl.multiple_of(grp * half, half), half)] if own_ else w_slot(src, m, grp)
        return pltpu.make_async_remote_copy(
            src_ref=origin, dst_ref=w_slot(src, m, grp),
            send_sem=send.at[src * 2 + m], recv_sem=recv.at[src * 2 + m],
            device_id={"sp": to}, device_id_type=MESH,
        )

    def w_side(src, m, g):
        return pltpu.make_async_remote_copy(
            src_ref=w_slot(src, m, g), dst_ref=w_slot(src, m, g),
            send_sem=wy_send.at[src * 2 + m], recv_sem=wy_recv.at[src * 2 + m],
            device_id={"grp": 1 - grp}, device_id_type=MESH,
        )

    def z_copy(src, dst, kind, j):
        at = span(kind, j)[2]
        return pltpu.make_async_remote_copy(
            src_ref=prompt.at[dst, part(kind, j, tp)], dst_ref=rows_in.at[src, part(kind, j, tp)],
            send_sem=z_send.at[dst * slots_per + at], recv_sem=z_recv.at[src * slots_per + at],
            device_id={"sp": dst}, device_id_type=MESH,
        )

    def side_copy(src, kind, j, q, to, send, recv):
        at = src * slots_per + span(kind, j)[2]
        return pltpu.make_async_remote_copy(
            src_ref=rows_in.at[src, part(kind, j, q)], dst_ref=rows_in.at[src, part(kind, j, q)],
            send_sem=send.at[at], recv_sem=recv.at[at],
            device_id={"tp": to}, device_id_type=MESH,
        )

    def take(src, kind, j):
        z_copy(src, me, kind, j).wait_recv()
        side_copy(src, kind, j, tp, across, x_send, x_recv).start()
        side_copy(src, kind, j, tp, sibling, d_send, d_recv).start()

    def relay(src, kind, j):
        side_copy(src, kind, j, across, across, x_send, x_recv).wait_recv()
        side_copy(src, kind, j, across, sibling, e_send, e_recv).start()

    def settle(src, kind, j):
        side_copy(src, kind, j, sibling, sibling, d_send, d_recv).wait_recv()
        side_copy(src, kind, j, far, sibling, e_send, e_recv).wait_recv()

    def send_all(items):
        for dst, kind, j in items:
            z_copy(me, dst, kind, j).start()

    for m in range(2):
        @pl.when(me + 1 < n)
        def _():
            w_hop(me, m, me + 1, wr_send, wr_recv, True).start()

        @pl.when(me > 0)
        def _():
            w_hop(me, m, me - 1, wl_send, wl_recv, True).start()

    for spot in range(n):
        @pl.when(me == spot)
        def _():
            send_all(right_plan(n, blocks, spot)[0])
            send_all(left_plan(n, blocks, spot)[0])

    small_in = [
        pltpu.make_async_copy(a, b, local.at[3 + i])
        for i, (a, b) in enumerate(
            ((query, q_in), (key_new, k_in), (value_new, v_in), (lam, lam_in), (gain, gain_in))
        )
    ]
    own_w = [
        pltpu.make_async_copy(
            mats[m],
            weights.at[pl.ds(pl.multiple_of(me * depth, depth), depth), pl.ds(m * cols, cols)],
            local.at[m],
        )
        for m in range(2)
    ]
    own_rows = pltpu.make_async_copy(prompt.at[me], rows_in.at[me], local.at[2])
    for copy in own_w + [own_rows] + small_in:
        copy.start()

    def weight_event(spot, src):
        for m in range(2):
            if src < spot:
                w_hop(src, m, me, wr_send, wr_recv, False).wait_recv()
                if spot + 1 < n:
                    w_hop(src, m, me + 1, wr_send, wr_recv, False).start()
            else:
                w_hop(src, m, me, wl_send, wl_recv, False).wait_recv()
                if spot > 0:
                    w_hop(src, m, me - 1, wl_send, wl_recv, False).start()
            w_side(src, m, grp).start()

    plans = [arrivals(n, blocks, spot) for spot in range(n)]
    aheads = [sum(kind == "big" for kind, _, _ in first) for first, _ in plans]
    orders = [
        [(s, j) for kind, s, j in first if kind == "big"] + [(s, j) for _, s, j in rest]
        for first, rest in plans
    ]
    total = len(orders[0])
    for spot in range(n):
        first = plans[spot][0]
        bigs = []

        @pl.when(me == spot)
        def _():
            lefts = [s for kind, s, _ in first if kind == "w" and s < spot]
            rights = [s for kind, s, _ in first if kind == "w" and s > spot]
            for kind, s, j in first:
                if kind == "w":
                    weight_event(spot, s)
                    if s < spot:
                        lefts.remove(s)
                        if not lefts:
                            send_all(right_plan(n, blocks, spot)[1])
                    else:
                        rights.remove(s)
                        if not rights:
                            send_all(left_plan(n, blocks, spot)[1])
                    continue
                take(s, kind, j)
                if kind == "big":
                    bigs.append((s, j))
                    if len(bigs) > 1:
                        relay(bigs[-2][0], "big", bigs[-2][1])
            relay(critical(n, spot), "fill", 0)
            if spot == 0:
                send_all(right_plan(n, blocks, spot)[1])
            if spot == n - 1:
                send_all(left_plan(n, blocks, spot)[1])

    for copy in small_in:
        copy.wait()

    def mine(ref):
        whole = ref[...].astype(jnp.float32)
        here = lax.broadcasted_iota(jnp.int32, whole.shape, 0) == me
        return jnp.sum(jnp.where(here, whole, 0.0), axis=0, keepdims=True)

    scale = HALF ** (-0.5)
    shape = (2 * heads, cols)
    row = lax.broadcasted_iota(jnp.int32, shape, 0)
    group = lax.broadcasted_iota(jnp.int32, shape, 1) // HALF
    chosen = jnp.where(row < heads, 2 * row, 2 * (row - heads) + 1) == group
    q_mat = jnp.where(chosen, jnp.broadcast_to(mine(q_in), shape), 0.0)
    fresh = jnp.sum(q_mat * mine(k_in), axis=1, keepdims=True) * scale
    q_low[...] = q_mat.astype(jnp.bfloat16)
    spread = (heads, heads)
    mix = jnp.sum(
        jnp.where(
            lax.broadcasted_iota(jnp.int32, spread, 0) == lax.broadcasted_iota(jnp.int32, spread, 1),
            jnp.broadcast_to(lam_in[...], spread), 0.0,
        ),
        axis=1, keepdims=True,
    )

    def project_rows(src, start, size):
        both = jnp.dot(
            rows_in[src, pl.ds(start, size), :], weights[...], preferred_element_type=jnp.float32
        ).astype(jnp.bfloat16)
        at = pl.ds(pl.multiple_of(src * piece + start, SMALL), size)
        keys[at, :] = both[:, :cols]
        values[at, :] = both[:, cols:]

    def score_rows(src, start, size):
        at = pl.multiple_of(src * piece + start, FILL)
        scores[:, pl.ds(at, size)] = lax.dot_general(
            q_low[...], keys[pl.ds(at, size), :], (((1,), (1,)), ((), ())),
            preferred_element_type=jnp.float32,
        ) * scale

    def compute(src, j):
        start = pl.multiple_of(j * BIG, BIG)
        project_rows(src, start, BIG)
        score_rows(src, start, BIG)

    picks = [by_spot([o[at][0] * blocks + o[at][1] for o in orders]) for at in range(total)]

    def order(k):
        pick = picks[0]
        for at in range(1, total):
            pick = jnp.where(k == at, picks[at], pick)
        return pick // blocks, lax.rem(pick, blocks)

    ahead = by_spot(aheads)

    def step(k, carry):
        @pl.when(k < total)
        def _():
            src, j = order(k)
            take_big(src, j)

        @pl.when(k - 1 < total)
        def _():
            src, j = order(k - 1)
            relay_big(src, j)

        @pl.when(k == ahead)
        def _():
            for step_ in range(1, n):
                src = lax.rem(me + step_, n)
                for m in range(2):
                    w_side(src, m, 1 - grp).wait_recv()
            for copy in own_w:
                copy.wait()
            own_rows.wait()

        @pl.when(k - ahead < blocks + ahead)
        def _():
            b = k - ahead
            src, j = order(b - blocks)
            foreign = b >= blocks

            @pl.when(foreign)
            def _():
                settle_big(src, j)

            compute(jnp.where(foreign, src, me), jnp.where(foreign, j, b))

        @pl.when(k - 2 >= ahead)
        def _():
            src, j = order(k - 2)
            settle_big(src, j)
            compute(src, j)

        return carry

    def dyn(j, q):
        quarter = BIG // 4
        return pl.ds(pl.multiple_of(j * BIG + q * quarter, quarter), quarter)

    def z_big(src, dst, j):
        return pltpu.make_async_remote_copy(
            src_ref=prompt.at[dst, dyn(j, tp)], dst_ref=rows_in.at[src, dyn(j, tp)],
            send_sem=z_send.at[dst * slots_per + j], recv_sem=z_recv.at[src * slots_per + j],
            device_id={"sp": dst}, device_id_type=MESH,
        )

    def side_big(src, j, q, to, send, recv):
        at = src * slots_per + j
        return pltpu.make_async_remote_copy(
            src_ref=rows_in.at[src, dyn(j, q)], dst_ref=rows_in.at[src, dyn(j, q)],
            send_sem=send.at[at], recv_sem=recv.at[at],
            device_id={"tp": to}, device_id_type=MESH,
        )

    def take_big(src, j):
        z_big(src, me, j).wait_recv()
        side_big(src, j, tp, across, x_send, x_recv).start()
        side_big(src, j, tp, sibling, d_send, d_recv).start()

    def relay_big(src, j):
        side_big(src, j, across, across, x_send, x_recv).wait_recv()
        side_big(src, j, across, sibling, e_send, e_recv).start()

    def settle_big(src, j):
        side_big(src, j, sibling, sibling, d_send, d_recv).wait_recv()
        side_big(src, j, far, sibling, e_send, e_recv).wait_recv()

    lax.fori_loop(ahead, total + 2, step, 0)

    last = piece - 2 * SMALL
    take(crit, "small", 0)
    settle(crit, "fill", 0)
    take(crit, "small", 1)
    relay(crit, "small", 0)
    settle(crit, "small", 0)
    project_rows(crit, piece - BIG, FILL + SMALL)
    score_rows(crit, piece - BIG, FILL)
    relay(crit, "small", 1)
    settle(crit, "small", 1)
    project_rows(crit, piece - SMALL, SMALL)
    score_rows(crit, last, 2 * SMALL)

    s = scores[...]
    top = jnp.maximum(jnp.max(s, axis=1, keepdims=True), fresh)
    e = jnp.exp(s - top)
    fresh_e = jnp.exp(fresh - top)
    sums = jnp.sum(e, axis=1, keepdims=True) + fresh_e
    w = e / sums
    fresh_w = fresh_e / sums
    mixed = (w[:heads] - mix * w[heads:]).astype(jnp.bfloat16)
    fresh_mixed = (fresh_w[:heads] - mix * fresh_w[heads:]).astype(jnp.bfloat16).astype(jnp.float32)
    o = jnp.dot(mixed, values[...], preferred_element_type=jnp.float32)
    o = o + fresh_mixed * mine(v_in)
    for h in range(heads):
        lanes = slice(h * VDIM, (h + 1) * VDIM)
        one = o[h:h + 1, lanes]
        mean = jnp.mean(one * one, axis=1, keepdims=True)
        own[:, lanes] = one * lax.rsqrt(mean + 1e-06) * gain_in[...]

    def row_copy(step_, src):
        return pltpu.make_async_remote_copy(
            src_ref=own, dst_ref=slots.at[src],
            send_sem=s_send.at[step_], recv_sem=s_recv.at[src],
            device_id={"sp": lax.rem(me + step_, n)}, device_id_type=MESH,
        )

    for step_ in range(1, n):
        row_copy(step_, me).start()

    for spot in range(n):
        @pl.when(me == spot)
        def _():
            for plan_ in (right_plan, left_plan):
                for dst, kind, j in sum(plan_(n, blocks, spot), []):
                    z_copy(me, dst, kind, j).wait_send()

    def drain(src, kind, j):
        side_copy(src, kind, j, tp, across, x_send, x_recv).wait_send()
        side_copy(src, kind, j, tp, sibling, d_send, d_recv).wait_send()
        side_copy(src, kind, j, across, sibling, e_send, e_recv).wait_send()

    def drain_big(k, carry):
        src, j = order(k)
        side_big(src, j, tp, across, x_send, x_recv).wait_send()
        side_big(src, j, tp, sibling, d_send, d_recv).wait_send()
        side_big(src, j, across, sibling, e_send, e_recv).wait_send()
        return carry

    lax.fori_loop(0, total, drain_big, 0)
    drain(crit, "fill", 0)
    drain(crit, "small", 0)
    drain(crit, "small", 1)
    for step_ in range(1, n):
        src = lax.rem(me + step_, n)
        for m in range(2):
            w_side(src, m, grp).wait_send()
    for d in range(n):
        for m in range(2):
            @pl.when((me - d >= 0) & (me + 1 < n))
            def _():
                w_hop(me - d, m, me + 1, wr_send, wr_recv, False).wait_send()

            @pl.when((me + d < n) & (me > 0))
            def _():
                w_hop(me + d, m, me - 1, wl_send, wl_recv, False).wait_send()

    for step_ in range(1, n):
        row_copy(step_, lax.rem(me + step_, n)).wait_recv()
    mine_row = own[...]
    for src in range(n):
        read[src:src + 1, :] = jnp.where(me == src, mine_row, slots[src]).astype(jnp.bfloat16)
    for step_ in range(1, n):
        row_copy(step_, me).wait_send()


def gather_project(n, prompt, w_key, w_value, query, key_new, value_new, mix_lambda, head_gain):
    count, piece, width = prompt.shape
    depth, cols = w_key.shape
    heads = mix_lambda.shape[0]
    dma = pltpu.SemaphoreType.DMA
    steps = n * (piece // BIG + 2)
    out = pltpu.VMEM((n * piece, cols), jnp.bfloat16)
    vmem = pl.BlockSpec(memory_space=pltpu.VMEM)
    hbm = pl.BlockSpec(memory_space=pltpu.HBM)
    f32, bf16 = jnp.float32, jnp.bfloat16
    return pl.pallas_call(
        functools.partial(gather_kernel, (n, piece)),
        out_shape=(out, out, pltpu.VMEM((n, cols), bf16)),
        in_specs=[hbm] * 8,
        out_specs=(vmem, vmem, vmem),
        scratch_shapes=[
            pltpu.VMEM((n, piece, width), bf16),
            pltpu.VMEM((n * depth, 2 * cols), bf16),
            pltpu.VMEM((2 * heads, n * piece), f32),
            pltpu.VMEM((2 * heads, cols), bf16),
            pltpu.VMEM((1, cols), f32),
            pltpu.VMEM((n, 1, cols), f32),
            pltpu.VMEM(query.shape, bf16),
            pltpu.VMEM(key_new.shape, bf16),
            pltpu.VMEM(value_new.shape, bf16),
            pltpu.VMEM((1, heads), f32),
            pltpu.VMEM((1, VDIM), f32),
        ]
        + [dma((steps,))] * 8
        + [dma((2 * n,))] * 6
        + [dma((n,))] * 2
        + [dma((8,))],
        compiler_params=pltpu.CompilerParams(
            collective_id=0, has_side_effects=True,
            vmem_limit_bytes=2**26 - 2**18 - 4 * n * piece * cols,
        ),
    )(
        prompt, w_key, w_value, query, key_new, value_new,
        mix_lambda[None, :], head_gain[None, :],
    )


def write_kernel(cuts, *refs):
    ins, outs, sem = refs[:3], refs[3:6], refs[6]
    copies = []
    for i in range(2):
        size = ins[i].shape[0] // cuts
        for c in range(cuts):
            at = pl.ds(c * size, size)
            copies.append((ins[i].at[at], outs[i].at[at]))
    copies.append((ins[2], outs[2]))
    copies = [pltpu.make_async_copy(a, b, sem.at[i]) for i, (a, b) in enumerate(copies)]
    for copy in copies:
        copy.start()
    for copy in copies:
        copy.wait()


def write_out(keys, values, read):
    cuts = 4
    hbm = pl.BlockSpec(memory_space=pltpu.HBM)
    vmem = pl.BlockSpec(memory_space=pltpu.VMEM)
    return pl.pallas_call(
        functools.partial(write_kernel, cuts),
        out_shape=tuple(jax.ShapeDtypeStruct(a.shape, a.dtype) for a in (keys, values, read)),
        in_specs=[vmem] * 3,
        out_specs=(hbm, hbm, hbm),
        scratch_shapes=[pltpu.SemaphoreType.DMA((2 * cuts + 1,))],
        compiler_params=pltpu.CompilerParams(vmem_limit_bytes=2**20),
    )(keys, values, read)


def fast_body(prompt, w_key, w_value, query_new, key_new, value_new, mix_lambda, head_gain):
    count, piece, width = prompt.shape
    n = lax.axis_size("sp")
    keys, values, read = write_out(
        *gather_project(
            n, prompt, w_key, w_value, query_new, key_new, value_new, mix_lambda, head_gain
        )
    )
    cols = keys.shape[-1]
    return (keys.reshape(1, n, piece, cols), values.reshape(1, n, piece, cols), read)


def choose(mesh):
    def run(prompt, *rest):
        sizes = dict(mesh.shape)
        count, piece, width = prompt.shape
        rows = rest[0].shape[0]
        fits = (
            sizes["grp"] == 2
            and sizes["tp"] == 4
            and sizes["sp"] == count
            and count % 2 == 0
            and count > 2
            and piece % BIG == 0
            and piece > 3 * BIG
            and rows % 32 == 0
            and count * piece * width * 2 <= 2**25
        )
        return (fast_body if fits else body)(prompt, *rest)

    return run


def solution(mesh):
    placed = (
        P("grp", "sp", None),
        P("sp", "tp"),
        P("sp", "tp"),
        P("grp", "tp"),
        P("grp", "tp"),
        P("grp", "tp"),
        P("tp"),
        P(),
    )
    return jax.shard_map(
        choose(mesh),
        mesh=mesh,
        in_specs=placed,
        out_specs=(
            P(("grp", "sp"), None, None, "tp"),
            P(("grp", "sp"), None, None, "tp"),
            P("grp", "tp"),
        ),
        check_vma=False,
    )
```

```python
import functools

import jax
import jax.numpy as jnp
from jax import lax
from jax.experimental import pallas as pl
from jax.experimental.pallas import tpu as pltpu
from jax.sharding import PartitionSpec as P

HALF = 64
VDIM = 128
MESH = pl.DeviceIdType.MESH
BIG = 256
MID = 128
SMALL = 64
START = 2


def combined_all(part, axis, combine):
    gathered = jax.tree.map(lambda a: lax.all_gather(a, axis), part)

    def take(source):
        return jax.tree.map(lambda a: lax.dynamic_index_in_dim(a, source, 0, False), gathered)

    return lax.fori_loop(
        1, lax.axis_size(axis), lambda source, state: combine(state, take(source)), take(0)
    )


def project(rows, w_key, w_value):
    keys = jnp.dot(
        rows, lax.all_gather(w_key, "sp", axis=0, tiled=True), preferred_element_type=jnp.float32
    )
    values = jnp.dot(
        rows, lax.all_gather(w_value, "sp", axis=0, tiled=True), preferred_element_type=jnp.float32
    )
    return (keys.astype(jnp.bfloat16), values.astype(jnp.bfloat16))


def score_maps(query, keys):
    count, span = (keys.shape[0], keys.shape[1])
    heads = query.shape[1] // (2 * HALF)
    q_parts = query.reshape(count, heads, 2, HALF)
    k_parts = keys.reshape(count, span, heads, 2, HALF)
    return jnp.einsum(
        "shmc,slhmc->shml", q_parts, k_parts, preferred_element_type=jnp.float32
    ) * HALF ** (-0.5)


def own_scores(query, fresh_key):
    count = query.shape[0]
    heads = query.shape[1] // (2 * HALF)
    q_parts = query.astype(jnp.float32).reshape(count, heads, 2, HALF)
    k_parts = fresh_key.astype(jnp.float32).reshape(count, heads, 2, HALF)
    return jnp.sum(q_parts * k_parts, axis=-1) * HALF ** (-0.5)


def finish(reads, head_gain):
    mean = jnp.mean(reads * reads, axis=-1, keepdims=True)
    normed = reads * lax.rsqrt(mean + 1e-06) * head_gain
    return normed.reshape(reads.shape[0], -1).astype(jnp.bfloat16)


def join_totals(first, second):
    top = jnp.maximum(first[0], second[0])
    return (top, first[1] * jnp.exp(first[0] - top) + second[1] * jnp.exp(second[0] - top))


def placed(part_rows, prompts, first, fill):
    base = jnp.full((prompts,) + part_rows.shape[1:], fill, jnp.float32)
    return lax.dynamic_update_slice_in_dim(base, part_rows, first, 0)


def cache_read(query_new, key_new, value_new, keys, values, mix_lambda, head_gain, first):
    count, span = (keys.shape[0], keys.shape[1])
    prompts = query_new.shape[0]
    heads = mix_lambda.shape[0]
    query = lax.dynamic_slice_in_dim(query_new, first, count, 0)
    scores = score_maps(query, keys)
    fresh_all = own_scores(query_new, key_new)
    fresh = lax.dynamic_slice_in_dim(fresh_all, first, count, 0)
    local_top = jnp.maximum(jnp.max(scores, axis=-1), fresh)
    local_total = jnp.sum(jnp.exp(scores - local_top[..., None]), axis=-1)
    top_all, cache_total = combined_all(
        (placed(local_top, prompts, first, -1e30), placed(local_total, prompts, first, 0.0)),
        "sp",
        join_totals,
    )
    own = jnp.exp(fresh_all - top_all)
    total_all = cache_total + own
    top = lax.dynamic_slice_in_dim(top_all, first, count, 0)
    total = lax.dynamic_slice_in_dim(total_all, first, count, 0)
    probs = jnp.exp(scores - top[..., None]) / total[..., None]
    mixed = (probs[:, :, 0] - mix_lambda[None, :, None] * probs[:, :, 1]).astype(jnp.bfloat16)
    value_parts = values.reshape(count, span, heads, VDIM)
    partial_value = jnp.einsum(
        "shl,slhv->shv", mixed, value_parts, preferred_element_type=jnp.float32
    )
    reads = lax.psum(placed(partial_value, prompts, first, 0.0), "sp")
    own_prob = own / total_all
    own_mixed = (own_prob[:, :, 0] - mix_lambda[None, :] * own_prob[:, :, 1]).astype(jnp.bfloat16)
    reads = reads + own_mixed.astype(jnp.float32)[..., None] * value_new.astype(
        jnp.float32
    ).reshape(prompts, heads, VDIM)
    return finish(reads, head_gain)


def block_read(
    query_new, key_new, value_new, key_cache, value_cache, mix_lambda, head_gain, spread
):
    blocks, sub = (key_cache.shape[1], key_cache.shape[2])
    first = lax.axis_index("sp") // spread
    keys = key_cache.reshape(1, blocks * sub, -1)
    values = value_cache.reshape(1, blocks * sub, -1)
    return cache_read(query_new, key_new, value_new, keys, values, mix_lambda, head_gain, first)


def body(prompt, w_key, w_value, query_new, key_new, value_new, mix_lambda, head_gain):
    count, piece, width = prompt.shape
    spread = lax.axis_size("sp") // count
    sub = piece // spread
    keys, values = project(prompt.reshape(count * piece, width), w_key, w_value)
    key_blocks = keys.reshape(count * spread, 1, sub, -1)
    value_blocks = values.reshape(count * spread, 1, sub, -1)
    key_cache, value_cache = (
        lax.all_to_all(key_blocks, "sp", split_axis=0, concat_axis=1, tiled=True),
        lax.all_to_all(value_blocks, "sp", split_axis=0, concat_axis=1, tiled=True),
    )
    first_read = block_read(
        query_new, key_new, value_new, key_cache, value_cache, mix_lambda, head_gain, spread
    )
    return (key_cache, value_cache, first_read)


def critical(n, spot):
    return n // 2 - 1 if spot >= n // 2 else n // 2


def tail_pieces(blocks):
    return [("big", j) for j in range(blocks - 2)] + [
        ("fill", 0), ("mid", 0), ("mid", 1), ("small", 0), ("small", 1)
    ]


def right_plan(n, blocks, src):
    far, near = n - 1, n // 2
    every = [("big", j) for j in range(blocks)]
    if src == 0:
        return [(1, *p) for p in every], [(d, *p) for p in every for d in (far, near)]
    if src == near:
        return [(far, *p) for p in every[:1]], [(far, *p) for p in every[1:]]
    if src == far:
        return [], []
    to_near = [(near, *p) for p in tail_pieces(blocks)]
    to_far = [(far, *p) for p in tail_pieces(blocks)]
    fill = blocks - 2
    early = [to_near.pop(fill)]
    late = to_near[:3] + to_far[:2] + to_near[3:4] + to_far[2:fill + 1]
    rest = zip(to_far[fill + 1:], to_near[4:])
    return early, late + [item for pair in rest for item in pair]


def left_plan(n, blocks, src):
    early, late = right_plan(n, blocks, n - 1 - src)
    flip = lambda items: [(n - 1 - dst, kind, j) for dst, kind, j in items]
    return flip(early), flip(late)


def arrivals(n, blocks, spot):
    if spot < n // 2:
        first, rest = arrivals(n, blocks, n - 1 - spot)
        flip = lambda items: [(kind, n - 1 - src, j) for kind, src, j in items]
        return flip(first), flip(rest)
    far = n - 1
    crit = [("big", 1, j) for j in range(blocks - 2)]
    through = [("big", 0, j) for j in range(blocks)]
    if spot == far:
        near = [("big", 2, j) for j in range(blocks)]
        first = [("w", 2, 0), near[0], ("w", 1, 0), ("w", 0, 0)]
        rest = [item for pair in zip(near[1:], through) for item in pair]
        return first, rest + through[blocks - 1:] + crit
    near = [("big", 3, j) for j in range(blocks)]
    first = [("w", 1, 0), ("w", 3, 0), ("fill", 1, 0), near[0], near[1], ("w", 0, 0)]
    rest = [near[2], crit[0], near[3], crit[1], near[4], crit[2], near[5]]
    return first, rest + near[6:] + through + crit[3:]


def gather_kernel(
    plan, prompt, w_key, w_value, query, key_new, value_new, lam, gain,
    keys, values, read,
    rows_in, weights, scores, q_low, own, slots,
    q_in, k_in, v_in, lam_in, gain_in,
    z_recv, x_recv, d_recv, w_recv, sent, met, local,
):
    n, piece = plan
    blocks = piece // BIG
    me = lax.axis_index("sp")
    tp = lax.axis_index("tp")
    grp = lax.axis_index("grp")
    across = lax.rem(tp + 2, 4)
    sibling = tp + 1 - 2 * lax.rem(tp, 2)
    far = lax.rem(sibling + 2, 4)
    depth, cols = w_key.shape
    heads = cols // VDIM
    half = depth // 2
    mats = (w_key, w_value)

    def by_spot(values_):
        pick = values_[0]
        for spot in range(1, n):
            pick = jnp.where(me == spot, values_[spot], pick)
        return pick

    crit = by_spot([critical(n, spot) for spot in range(n)])

    def span(kind, j):
        if kind == "big":
            return j * BIG, BIG
        if kind == "small":
            return piece - (2 - j) * SMALL, SMALL
        return piece - 2 * BIG + (0 if kind == "fill" else 1 + j) * MID, MID

    def flag(src, kind, j):
        if kind == "small":
            return n * blocks + 1 + j
        if kind == "big":
            return src * blocks + j
        return n * blocks if (kind, j) == ("mid", 1) else src * blocks + blocks - 2 + (kind == "mid")

    def part(kind, j, q):
        start, size = span(kind, j)
        quarter = size // 4
        return pl.ds(pl.multiple_of(start + q * quarter, quarter), quarter)

    barrier = pltpu.get_barrier_semaphore()
    for step in range(1, n):
        pl.semaphore_signal(
            barrier, inc=1, device_id={"sp": lax.rem(me + step, n)}, device_id_type=MESH
        )
    pl.semaphore_signal(barrier, inc=1, device_id={"tp": across}, device_id_type=MESH)
    pl.semaphore_signal(barrier, inc=1, device_id={"tp": sibling}, device_id_type=MESH)
    pl.semaphore_signal(barrier, inc=1, device_id={"grp": 1 - grp}, device_id_type=MESH)
    pl.semaphore_wait(barrier, n + 2)

    def w_slot(src, m, g):
        return weights.at[pl.ds(pl.multiple_of(src * depth + g * half, half), half),
                          pl.ds(m * cols, cols)]

    def w_hop(src, m, to, own_):
        origin = mats[m].at[pl.ds(pl.multiple_of(grp * half, half), half)] if own_ else w_slot(src, m, grp)
        return pltpu.make_async_remote_copy(
            src_ref=origin, dst_ref=w_slot(src, m, grp),
            send_sem=sent.at[0], recv_sem=w_recv.at[src * 2 + m],
            device_id={"sp": to}, device_id_type=MESH,
        )

    def w_side(src, m, g):
        return pltpu.make_async_remote_copy(
            src_ref=w_slot(src, m, g), dst_ref=w_slot(src, m, g),
            send_sem=sent.at[1], recv_sem=met.at[0],
            device_id={"grp": 1 - grp}, device_id_type=MESH,
        )

    def w_all(count):
        block = weights.at[pl.ds(0, count * half)]
        return pltpu.make_async_remote_copy(
            src_ref=block, dst_ref=block, send_sem=sent.at[1], recv_sem=met.at[0],
            device_id={"grp": 1 - grp}, device_id_type=MESH,
        )

    def z_copy(src, dst, kind, j):
        return pltpu.make_async_remote_copy(
            src_ref=prompt.at[dst, part(kind, j, tp)], dst_ref=rows_in.at[src, part(kind, j, tp)],
            send_sem=sent.at[2], recv_sem=z_recv.at[flag(src, kind, j)],
            device_id={"sp": dst}, device_id_type=MESH,
        )

    def side_copy(src, kind, j, q, to, send, recv):
        return pltpu.make_async_remote_copy(
            src_ref=rows_in.at[src, part(kind, j, q)], dst_ref=rows_in.at[src, part(kind, j, q)],
            send_sem=sent.at[send], recv_sem=recv.at[flag(src, kind, j)],
            device_id={"tp": to}, device_id_type=MESH,
        )

    def both_halves(src, start, size, at):
        rows = rows_in.at[src, pl.ds(pl.multiple_of(start, size), size)]
        return pltpu.make_async_remote_copy(
            src_ref=rows, dst_ref=rows, send_sem=sent.at[4], recv_sem=d_recv.at[at],
            device_id={"tp": sibling}, device_id_type=MESH,
        )

    def take(src, kind, j):
        z_copy(src, me, kind, j).wait_recv()
        side_copy(src, kind, j, tp, across, 3, x_recv).start()
        side_copy(src, kind, j, tp, sibling, 4, d_recv).start()

    def relay(src, kind, j):
        side_copy(src, kind, j, across, across, 3, x_recv).wait_recv()
        side_copy(src, kind, j, across, sibling, 5, d_recv).start()

    def settle(src, kind, j):
        start, size = span(kind, j)
        both_halves(src, start, size // 2, flag(src, kind, j)).wait_recv()

    def send_all(items):
        for dst, kind, j in items:
            z_copy(me, dst, kind, j).start()

    for m in range(2):
        @pl.when(me + 1 < n)
        def _():
            w_hop(me, m, me + 1, True).start()

        @pl.when(me > 0)
        def _():
            w_hop(me, m, me - 1, True).start()

    for spot in range(n):
        @pl.when(me == spot)
        def _():
            send_all(right_plan(n, blocks, spot)[0])
            send_all(left_plan(n, blocks, spot)[0])

    small_in = [
        pltpu.make_async_copy(a, b, local.at[3 + i])
        for i, (a, b) in enumerate(
            ((query, q_in), (key_new, k_in), (value_new, v_in), (lam, lam_in), (gain, gain_in))
        )
    ]
    own_w = [
        pltpu.make_async_copy(
            mats[m],
            weights.at[pl.ds(pl.multiple_of(me * depth, depth), depth), pl.ds(m * cols, cols)],
            local.at[m],
        )
        for m in range(2)
    ]
    own_rows = pltpu.make_async_copy(prompt.at[me], rows_in.at[me], local.at[2])
    for copy in own_w + [own_rows] + small_in:
        copy.start()

    def weight_event(spot, src):
        for m in range(2):
            if src < spot:
                w_hop(src, m, me, False).wait_recv()
                if spot + 1 < n:
                    w_hop(src, m, me + 1, False).start()
            else:
                w_hop(src, m, me, False).wait_recv()
                if spot > 0:
                    w_hop(src, m, me - 1, False).start()
            w_side(src, m, grp).start()

    plans = [arrivals(n, blocks, spot) for spot in range(n)]
    aheads = [sum(kind == "big" for kind, _, _ in first) for first, _ in plans]
    orders = [
        [(s, j) for kind, s, j in first if kind == "big"] + [(s, j) for _, s, j in rest]
        for first, rest in plans
    ]
    total = len(orders[0])
    for spot in range(n):
        first = plans[spot][0]
        bigs = []

        @pl.when(me == spot)
        def _():
            lefts = [s for kind, s, _ in first if kind == "w" and s < spot]
            rights = [s for kind, s, _ in first if kind == "w" and s > spot]
            for kind, s, j in first:
                if kind == "w":
                    weight_event(spot, s)
                    if s < spot:
                        lefts.remove(s)
                        if not lefts:
                            send_all(right_plan(n, blocks, spot)[1])
                    else:
                        rights.remove(s)
                        if not rights:
                            send_all(left_plan(n, blocks, spot)[1])
                    continue
                take(s, kind, j)
                if kind == "big":
                    bigs.append((s, j))
                    if len(bigs) > 1:
                        relay(bigs[-2][0], "big", bigs[-2][1])
            if any(kind == "fill" for kind, _, _ in first):
                relay(critical(n, spot), "fill", 0)
            if spot == 0:
                send_all(right_plan(n, blocks, spot)[1])
            if spot == n - 1:
                send_all(left_plan(n, blocks, spot)[1])

    for copy in small_in:
        copy.wait()

    def mine(ref):
        whole = ref[...].astype(jnp.float32)
        here = lax.broadcasted_iota(jnp.int32, whole.shape, 0) == me
        return jnp.sum(jnp.where(here, whole, 0.0), axis=0, keepdims=True)

    scale = HALF ** (-0.5)
    shape = (2 * heads, cols)
    row = lax.broadcasted_iota(jnp.int32, shape, 0)
    group = lax.broadcasted_iota(jnp.int32, shape, 1) // HALF
    chosen = jnp.where(row < heads, 2 * row, 2 * (row - heads) + 1) == group
    q_mat = jnp.where(chosen, jnp.broadcast_to(mine(q_in), shape), 0.0)
    fresh = jnp.sum(q_mat * mine(k_in), axis=1, keepdims=True) * scale
    q_low[...] = q_mat.astype(jnp.bfloat16)
    spread = (heads, heads)
    mix = jnp.sum(
        jnp.where(
            lax.broadcasted_iota(jnp.int32, spread, 0) == lax.broadcasted_iota(jnp.int32, spread, 1),
            jnp.broadcast_to(lam_in[...], spread), 0.0,
        ),
        axis=1, keepdims=True,
    )

    def project_rows(src, start, size):
        both = jnp.dot(
            rows_in[src, pl.ds(start, size), :], weights[...], preferred_element_type=jnp.float32
        ).astype(jnp.bfloat16)
        at = pl.ds(pl.multiple_of(src * piece + start, SMALL), size)
        keys[at, :] = both[:, :cols]
        values[at, :] = both[:, cols:]

    def score_rows(src, start, size):
        at = pl.multiple_of(src * piece + start, MID)
        scores[:, pl.ds(at, size)] = lax.dot_general(
            q_low[...], keys[pl.ds(at, size), :], (((1,), (1,)), ((), ())),
            preferred_element_type=jnp.float32,
        ) * scale

    def compute(src, j):
        start = pl.multiple_of(j * BIG, BIG)
        project_rows(src, start, BIG)
        score_rows(src, start, BIG)

    picks = [by_spot([o[at][0] * blocks + o[at][1] for o in orders]) for at in range(total)]

    def order(k):
        pick = picks[0]
        for at in range(1, total):
            pick = jnp.where(k == at, picks[at], pick)
        return pick // blocks, lax.rem(pick, blocks)

    ahead = by_spot(aheads)

    def step(k, carry):
        src, j = order(k)
        take_big(src, j)
        src, j = order(k - 1)
        relay_big(src, j)

        @pl.when(k == ahead + START)
        def _():
            w_all(n - 1).wait_recv()
            for copy in own_w:
                copy.wait()
            own_rows.wait()

        b = k - ahead - START

        @pl.when((b >= 0) & (b < blocks + ahead))
        def _():
            src, j = order(b - blocks)
            foreign = b >= blocks

            @pl.when(foreign)
            def _():
                settle_big(src, j)

            compute(jnp.where(foreign, src, me), jnp.where(foreign, j, b))

        @pl.when(k - 2 >= ahead)
        def _():
            src, j = order(k - 2)
            settle_big(src, j)
            compute(src, j)

        return carry

    def dyn(j, q):
        quarter = BIG // 4
        return pl.ds(pl.multiple_of(j * BIG + q * quarter, quarter), quarter)

    def z_big(src, dst, j):
        return pltpu.make_async_remote_copy(
            src_ref=prompt.at[dst, dyn(j, tp)], dst_ref=rows_in.at[src, dyn(j, tp)],
            send_sem=sent.at[2], recv_sem=z_recv.at[src * blocks + j],
            device_id={"sp": dst}, device_id_type=MESH,
        )

    def side_big(src, j, q, to, send, recv):
        return pltpu.make_async_remote_copy(
            src_ref=rows_in.at[src, dyn(j, q)], dst_ref=rows_in.at[src, dyn(j, q)],
            send_sem=sent.at[send], recv_sem=recv.at[src * blocks + j],
            device_id={"tp": to}, device_id_type=MESH,
        )

    def take_big(src, j):
        z_big(src, me, j).wait_recv()
        side_big(src, j, tp, across, 3, x_recv).start()
        side_big(src, j, tp, sibling, 4, d_recv).start()

    def relay_big(src, j):
        side_big(src, j, across, across, 3, x_recv).wait_recv()
        side_big(src, j, across, sibling, 5, d_recv).start()

    def settle_big(src, j):
        both_halves(src, j * BIG, BIG // 2, src * blocks + j).wait_recv()

    lax.fori_loop(ahead, total, step, 0)

    late_fill = (me == 0) | (me == n - 1)

    @pl.when(late_fill)
    def _():
        take(crit, "fill", 0)

    src, j = order(total - 1)
    relay_big(src, j)

    def last_bigs(k, carry):
        src, j = order(k)

        @pl.when(k < total)
        def _():
            settle_big(src, j)

        @pl.when(k == total - 1)
        def _():
            take(crit, "mid", 0)

            @pl.when(late_fill)
            def _():
                relay(crit, "fill", 0)

        @pl.when(k == total)
        def _():
            take(crit, "mid", 1)
            relay(crit, "mid", 0)
            take(crit, "small", 0)
            settle(crit, "fill", 0)
            settle(crit, "mid", 0)

        final = k == total
        compute(jnp.where(final, crit, src), jnp.where(final, blocks - 2, j))
        return carry

    lax.fori_loop(total - 2, total + 1, last_bigs, 0)

    take(crit, "small", 1)
    relay(crit, "mid", 1)
    relay(crit, "small", 0)
    settle(crit, "mid", 1)
    settle(crit, "small", 0)
    project_rows(crit, piece - BIG, MID + SMALL)
    score_rows(crit, piece - BIG, MID)
    relay(crit, "small", 1)
    settle(crit, "small", 1)
    project_rows(crit, piece - SMALL, SMALL)
    score_rows(crit, piece - 2 * SMALL, 2 * SMALL)

    s = scores[...]
    top = jnp.maximum(jnp.max(s, axis=1, keepdims=True), fresh)
    e = jnp.exp(s - top)
    fresh_e = jnp.exp(fresh - top)
    sums = jnp.sum(e, axis=1, keepdims=True) + fresh_e
    w = e / sums
    fresh_w = fresh_e / sums
    mixed = (w[:heads] - mix * w[heads:]).astype(jnp.bfloat16)
    fresh_mixed = (fresh_w[:heads] - mix * fresh_w[heads:]).astype(jnp.bfloat16).astype(jnp.float32)
    o = jnp.dot(mixed, values[...], preferred_element_type=jnp.float32)
    o = o + fresh_mixed * mine(v_in)
    for h in range(heads):
        lanes = slice(h * VDIM, (h + 1) * VDIM)
        one = o[h:h + 1, lanes]
        mean = jnp.mean(one * one, axis=1, keepdims=True)
        own[:, lanes] = one * lax.rsqrt(mean + 1e-06) * gain_in[...]

    def row_copy(step_, src):
        return pltpu.make_async_remote_copy(
            src_ref=own, dst_ref=slots.at[src], send_sem=sent.at[6], recv_sem=met.at[1],
            device_id={"sp": lax.rem(me + step_, n)}, device_id_type=MESH,
        )

    for step_ in range(1, n):
        row_copy(step_, me).start()

    def all_sent(block, at):
        pltpu.make_async_remote_copy(
            src_ref=block, dst_ref=block, send_sem=sent.at[at], recv_sem=met.at[1],
            device_id={"sp": lax.rem(me + 1, n)}, device_id_type=MESH,
        ).wait_send()

    for at in range(2, 6):
        all_sent(rows_in.at[0, pl.ds(0, (n - 1) * piece // 4)], at)
    w_all(n - 1).wait_send()
    inner = (me > 0) & (me + 1 < n)

    @pl.when(inner)
    def _():
        all_sent(weights.at[pl.ds(0, (n + 1) * half)], 0)

    @pl.when(jnp.logical_not(inner))
    def _():
        all_sent(weights.at[pl.ds(0, half)], 0)

    others = slots.at[pl.ds(0, n - 1)]
    pltpu.make_async_remote_copy(
        src_ref=others, dst_ref=others, send_sem=sent.at[6], recv_sem=met.at[1],
        device_id={"sp": lax.rem(me + 1, n)}, device_id_type=MESH,
    ).wait_recv()
    mine_row = own[...]
    for src in range(n):
        read[src:src + 1, :] = jnp.where(me == src, mine_row, slots[src]).astype(jnp.bfloat16)
    all_sent(others, 6)


def gather_project(n, prompt, w_key, w_value, query, key_new, value_new, mix_lambda, head_gain):
    count, piece, width = prompt.shape
    depth, cols = w_key.shape
    heads = mix_lambda.shape[0]
    dma = pltpu.SemaphoreType.DMA
    steps = n * (piece // BIG) + 3
    out = pltpu.VMEM((n * piece, cols), jnp.bfloat16)
    vmem = pl.BlockSpec(memory_space=pltpu.VMEM)
    hbm = pl.BlockSpec(memory_space=pltpu.HBM)
    f32, bf16 = jnp.float32, jnp.bfloat16
    return pl.pallas_call(
        functools.partial(gather_kernel, (n, piece)),
        out_shape=(out, out, pltpu.VMEM((n, cols), bf16)),
        in_specs=[hbm] * 8,
        out_specs=(vmem, vmem, vmem),
        scratch_shapes=[
            pltpu.VMEM((n, piece, width), bf16),
            pltpu.VMEM((n * depth, 2 * cols), bf16),
            pltpu.VMEM((2 * heads, n * piece), f32),
            pltpu.VMEM((2 * heads, cols), bf16),
            pltpu.VMEM((1, cols), f32),
            pltpu.VMEM((n, 1, cols), f32),
            pltpu.VMEM(query.shape, bf16),
            pltpu.VMEM(key_new.shape, bf16),
            pltpu.VMEM(value_new.shape, bf16),
            pltpu.VMEM((1, heads), f32),
            pltpu.VMEM((1, VDIM), f32),
        ]
        + [dma((steps,))] * 3
        + [dma((2 * n,)), dma((7,)), dma((2,)), dma((8,))],
        compiler_params=pltpu.CompilerParams(
            collective_id=0, has_side_effects=True,
            vmem_limit_bytes=2**26 - 2**18 - 4 * n * piece * cols,
        ),
    )(
        prompt, w_key, w_value, query, key_new, value_new,
        mix_lambda[None, :], head_gain[None, :],
    )


def write_kernel(cuts, *refs):
    ins, outs, sem = refs[:3], refs[3:6], refs[6]
    copies = []
    for i in range(2):
        size = ins[i].shape[0] // cuts
        for c in range(cuts):
            at = pl.ds(c * size, size)
            copies.append((ins[i].at[at], outs[i].at[at]))
    copies.append((ins[2], outs[2]))
    copies = [pltpu.make_async_copy(a, b, sem.at[i]) for i, (a, b) in enumerate(copies)]
    for copy in copies:
        copy.start()
    for copy in copies:
        copy.wait()


def write_out(keys, values, read):
    cuts = 4
    hbm = pl.BlockSpec(memory_space=pltpu.HBM)
    vmem = pl.BlockSpec(memory_space=pltpu.VMEM)
    return pl.pallas_call(
        functools.partial(write_kernel, cuts),
        out_shape=tuple(jax.ShapeDtypeStruct(a.shape, a.dtype) for a in (keys, values, read)),
        in_specs=[vmem] * 3,
        out_specs=(hbm, hbm, hbm),
        scratch_shapes=[pltpu.SemaphoreType.DMA((2 * cuts + 1,))],
        compiler_params=pltpu.CompilerParams(vmem_limit_bytes=2**20),
    )(keys, values, read)


def fast_body(prompt, w_key, w_value, query_new, key_new, value_new, mix_lambda, head_gain):
    count, piece, width = prompt.shape
    n = lax.axis_size("sp")
    keys, values, read = write_out(
        *gather_project(
            n, prompt, w_key, w_value, query_new, key_new, value_new, mix_lambda, head_gain
        )
    )
    cols = keys.shape[-1]
    return (keys.reshape(1, n, piece, cols), values.reshape(1, n, piece, cols), read)


def choose(mesh):
    def run(prompt, *rest):
        sizes = dict(mesh.shape)
        count, piece, width = prompt.shape
        rows = rest[0].shape[0]
        fits = (
            sizes["grp"] == 2
            and sizes["tp"] == 4
            and sizes["sp"] == count
            and count == 4
            and piece % BIG == 0
            and piece >= 6 * BIG
            and rows % 32 == 0
            and count * piece * width * 2 <= 2**25
        )
        return (fast_body if fits else body)(prompt, *rest)

    return run


def solution(mesh):
    placed = (
        P("grp", "sp", None),
        P("sp", "tp"),
        P("sp", "tp"),
        P("grp", "tp"),
        P("grp", "tp"),
        P("grp", "tp"),
        P("tp"),
        P(),
    )
    return jax.shard_map(
        choose(mesh),
        mesh=mesh,
        in_specs=placed,
        out_specs=(
            P(("grp", "sp"), None, None, "tp"),
            P(("grp", "sp"), None, None, "tp"),
            P("grp", "tp"),
        ),
        check_vma=False,
    )
```

```python
import functools

import jax
import jax.numpy as jnp
from jax import lax
from jax.experimental import pallas as pl
from jax.experimental.pallas import tpu as pltpu
from jax.sharding import PartitionSpec as P

HALF = 64
VDIM = 128
MESH = pl.DeviceIdType.MESH
BIG = 256
TAIL = (128, 128, 128, 64, 32, 32)
START = 2
HOLD = 3


def combined_all(part, axis, combine):
    gathered = jax.tree.map(lambda a: lax.all_gather(a, axis), part)

    def take(source):
        return jax.tree.map(lambda a: lax.dynamic_index_in_dim(a, source, 0, False), gathered)

    return lax.fori_loop(
        1, lax.axis_size(axis), lambda source, state: combine(state, take(source)), take(0)
    )


def project(rows, w_key, w_value):
    keys = jnp.dot(
        rows, lax.all_gather(w_key, "sp", axis=0, tiled=True), preferred_element_type=jnp.float32
    )
    values = jnp.dot(
        rows, lax.all_gather(w_value, "sp", axis=0, tiled=True), preferred_element_type=jnp.float32
    )
    return (keys.astype(jnp.bfloat16), values.astype(jnp.bfloat16))


def score_maps(query, keys):
    count, span = (keys.shape[0], keys.shape[1])
    heads = query.shape[1] // (2 * HALF)
    q_parts = query.reshape(count, heads, 2, HALF)
    k_parts = keys.reshape(count, span, heads, 2, HALF)
    return jnp.einsum(
        "shmc,slhmc->shml", q_parts, k_parts, preferred_element_type=jnp.float32
    ) * HALF ** (-0.5)


def own_scores(query, fresh_key):
    count = query.shape[0]
    heads = query.shape[1] // (2 * HALF)
    q_parts = query.astype(jnp.float32).reshape(count, heads, 2, HALF)
    k_parts = fresh_key.astype(jnp.float32).reshape(count, heads, 2, HALF)
    return jnp.sum(q_parts * k_parts, axis=-1) * HALF ** (-0.5)


def finish(reads, head_gain):
    mean = jnp.mean(reads * reads, axis=-1, keepdims=True)
    normed = reads * lax.rsqrt(mean + 1e-06) * head_gain
    return normed.reshape(reads.shape[0], -1).astype(jnp.bfloat16)


def join_totals(first, second):
    top = jnp.maximum(first[0], second[0])
    return (top, first[1] * jnp.exp(first[0] - top) + second[1] * jnp.exp(second[0] - top))


def placed(part_rows, prompts, first, fill):
    base = jnp.full((prompts,) + part_rows.shape[1:], fill, jnp.float32)
    return lax.dynamic_update_slice_in_dim(base, part_rows, first, 0)


def cache_read(query_new, key_new, value_new, keys, values, mix_lambda, head_gain, first):
    count, span = (keys.shape[0], keys.shape[1])
    prompts = query_new.shape[0]
    heads = mix_lambda.shape[0]
    query = lax.dynamic_slice_in_dim(query_new, first, count, 0)
    scores = score_maps(query, keys)
    fresh_all = own_scores(query_new, key_new)
    fresh = lax.dynamic_slice_in_dim(fresh_all, first, count, 0)
    local_top = jnp.maximum(jnp.max(scores, axis=-1), fresh)
    local_total = jnp.sum(jnp.exp(scores - local_top[..., None]), axis=-1)
    top_all, cache_total = combined_all(
        (placed(local_top, prompts, first, -1e30), placed(local_total, prompts, first, 0.0)),
        "sp",
        join_totals,
    )
    own = jnp.exp(fresh_all - top_all)
    total_all = cache_total + own
    top = lax.dynamic_slice_in_dim(top_all, first, count, 0)
    total = lax.dynamic_slice_in_dim(total_all, first, count, 0)
    probs = jnp.exp(scores - top[..., None]) / total[..., None]
    mixed = (probs[:, :, 0] - mix_lambda[None, :, None] * probs[:, :, 1]).astype(jnp.bfloat16)
    value_parts = values.reshape(count, span, heads, VDIM)
    partial_value = jnp.einsum(
        "shl,slhv->shv", mixed, value_parts, preferred_element_type=jnp.float32
    )
    reads = lax.psum(placed(partial_value, prompts, first, 0.0), "sp")
    own_prob = own / total_all
    own_mixed = (own_prob[:, :, 0] - mix_lambda[None, :] * own_prob[:, :, 1]).astype(jnp.bfloat16)
    reads = reads + own_mixed.astype(jnp.float32)[..., None] * value_new.astype(
        jnp.float32
    ).reshape(prompts, heads, VDIM)
    return finish(reads, head_gain)


def block_read(
    query_new, key_new, value_new, key_cache, value_cache, mix_lambda, head_gain, spread
):
    blocks, sub = (key_cache.shape[1], key_cache.shape[2])
    first = lax.axis_index("sp") // spread
    keys = key_cache.reshape(1, blocks * sub, -1)
    values = value_cache.reshape(1, blocks * sub, -1)
    return cache_read(query_new, key_new, value_new, keys, values, mix_lambda, head_gain, first)


def body(prompt, w_key, w_value, query_new, key_new, value_new, mix_lambda, head_gain):
    count, piece, width = prompt.shape
    spread = lax.axis_size("sp") // count
    sub = piece // spread
    keys, values = project(prompt.reshape(count * piece, width), w_key, w_value)
    key_blocks = keys.reshape(count * spread, 1, sub, -1)
    value_blocks = values.reshape(count * spread, 1, sub, -1)
    key_cache, value_cache = (
        lax.all_to_all(key_blocks, "sp", split_axis=0, concat_axis=1, tiled=True),
        lax.all_to_all(value_blocks, "sp", split_axis=0, concat_axis=1, tiled=True),
    )
    first_read = block_read(
        query_new, key_new, value_new, key_cache, value_cache, mix_lambda, head_gain, spread
    )
    return (key_cache, value_cache, first_read)


def critical(n, spot):
    return n // 2 - 1 if spot >= n // 2 else n // 2


def tail_pieces(blocks):
    return [("big", j) for j in range(blocks - 2)] + [("tail", j) for j in range(len(TAIL))]


def right_plan(n, blocks, src):
    far, near = n - 1, n // 2
    every = [("big", j) for j in range(blocks)]
    if src == 0:
        return [(1, *p) for p in every], [(d, *p) for p in every for d in (far, near)]
    if src == near:
        return [(far, *p) for p in every[:1]], [(far, *p) for p in every[1:]]
    if src == far:
        return [], []
    to_near = [(near, *p) for p in tail_pieces(blocks)]
    to_far = [(far, *p) for p in tail_pieces(blocks)]
    fill = blocks - 2
    early = [to_near.pop(fill)]
    late = to_near[:3] + to_far[:2] + to_near[3:4] + to_far[2:fill + 1]
    rest = zip(to_far[fill + 1:], to_near[4:])
    return early, late + [item for pair in rest for item in pair]


def left_plan(n, blocks, src):
    early, late = right_plan(n, blocks, n - 1 - src)
    flip = lambda items: [(n - 1 - dst, kind, j) for dst, kind, j in items]
    return flip(early), flip(late)


def arrivals(n, blocks, spot):
    if spot < n // 2:
        first, rest = arrivals(n, blocks, n - 1 - spot)
        flip = lambda items: [(kind, n - 1 - src, j) for kind, src, j in items]
        return flip(first), flip(rest)
    far = n - 1
    crit = [("big", 1, j) for j in range(blocks - 2)]
    through = [("big", 0, j) for j in range(blocks)]
    if spot == far:
        near = [("big", 2, j) for j in range(blocks)]
        first = [("w", 2, 0), near[0], ("w", 1, 0), ("w", 0, 0)]
        rest = [item for pair in zip(near[1:], through) for item in pair]
        return first, rest + through[blocks - 1:] + crit
    near = [("big", 3, j) for j in range(blocks)]
    first = [("w", 1, 0), ("w", 3, 0), ("tail", 1, 0), near[0], near[1], ("w", 0, 0)]
    rest = [near[2], crit[0], near[3], crit[1], near[4], crit[2], near[5]]
    return first, rest + near[6:] + through + crit[3:]


def gather_kernel(
    plan, prompt, w_key, w_value, query, key_new, value_new, lam, gain,
    keys, values, read,
    rows_in, weights, scores, q_low, own, slots,
    q_in, k_in, v_in, lam_in, gain_in,
    z_recv, x_recv, d_recv, w_recv, sent, met, local,
):
    n, piece = plan
    blocks = piece // BIG
    me = lax.axis_index("sp")
    tp = lax.axis_index("tp")
    grp = lax.axis_index("grp")
    across = lax.rem(tp + 2, 4)
    sibling = tp + 1 - 2 * lax.rem(tp, 2)
    far = lax.rem(sibling + 2, 4)
    depth, cols = w_key.shape
    heads = cols // VDIM
    half = depth // 2
    mats = (w_key, w_value)

    def by_spot(values_):
        pick = values_[0]
        for spot in range(1, n):
            pick = jnp.where(me == spot, values_[spot], pick)
        return pick

    crit = by_spot([critical(n, spot) for spot in range(n)])

    def span(kind, j):
        if kind == "big":
            return j * BIG, BIG
        return piece - sum(TAIL[j:]), TAIL[j]

    def flag(src, kind, j):
        if kind == "big":
            return src * blocks + j
        return src * blocks + blocks - 2 + j if j < 2 else n * blocks + j - 2

    def part(kind, j, q):
        start, size = span(kind, j)
        quarter = size // 4
        return pl.ds(pl.multiple_of(start + q * quarter, quarter), quarter)

    barrier = pltpu.get_barrier_semaphore()

    @pl.when(me + 1 < n)
    def _():
        pl.semaphore_signal(barrier, inc=1, device_id={"sp": me + 1}, device_id_type=MESH)

    @pl.when(me > 0)
    def _():
        pl.semaphore_signal(barrier, inc=1, device_id={"sp": me - 1}, device_id_type=MESH)

    pl.semaphore_signal(barrier, inc=1, device_id={"tp": across}, device_id_type=MESH)
    pl.semaphore_signal(barrier, inc=1, device_id={"tp": sibling}, device_id_type=MESH)
    pl.semaphore_signal(barrier, inc=1, device_id={"grp": 1 - grp}, device_id_type=MESH)
    pl.semaphore_wait(barrier, jnp.where((me > 0) & (me + 1 < n), 5, 4))

    def w_slot(src, m, g):
        return weights.at[pl.ds(pl.multiple_of(src * depth + g * half, half), half),
                          pl.ds(m * cols, cols)]

    def w_hop(src, m, to, own_):
        origin = mats[m].at[pl.ds(pl.multiple_of(grp * half, half), half)] if own_ else w_slot(src, m, grp)
        return pltpu.make_async_remote_copy(
            src_ref=origin, dst_ref=w_slot(src, m, grp),
            send_sem=sent.at[0], recv_sem=w_recv.at[src * 2 + m],
            device_id={"sp": to}, device_id_type=MESH,
        )

    def w_side(src, m, g):
        return pltpu.make_async_remote_copy(
            src_ref=w_slot(src, m, g), dst_ref=w_slot(src, m, g),
            send_sem=sent.at[1], recv_sem=met.at[0],
            device_id={"grp": 1 - grp}, device_id_type=MESH,
        )

    def w_all(count):
        block = weights.at[pl.ds(0, count * half)]
        return pltpu.make_async_remote_copy(
            src_ref=block, dst_ref=block, send_sem=sent.at[1], recv_sem=met.at[0],
            device_id={"grp": 1 - grp}, device_id_type=MESH,
        )

    def z_copy(src, dst, kind, j):
        return pltpu.make_async_remote_copy(
            src_ref=prompt.at[dst, part(kind, j, tp)], dst_ref=rows_in.at[src, part(kind, j, tp)],
            send_sem=sent.at[2], recv_sem=z_recv.at[flag(src, kind, j)],
            device_id={"sp": dst}, device_id_type=MESH,
        )

    def side_copy(src, kind, j, q, to, send, recv):
        return pltpu.make_async_remote_copy(
            src_ref=rows_in.at[src, part(kind, j, q)], dst_ref=rows_in.at[src, part(kind, j, q)],
            send_sem=sent.at[send], recv_sem=recv.at[flag(src, kind, j)],
            device_id={"tp": to}, device_id_type=MESH,
        )

    def both_halves(src, start, size, at):
        rows = rows_in.at[src, pl.ds(pl.multiple_of(start, size), size)]
        return pltpu.make_async_remote_copy(
            src_ref=rows, dst_ref=rows, send_sem=sent.at[4], recv_sem=d_recv.at[at],
            device_id={"tp": sibling}, device_id_type=MESH,
        )

    def take(src, kind, j):
        z_copy(src, me, kind, j).wait_recv()
        side_copy(src, kind, j, tp, across, 3, x_recv).start()
        side_copy(src, kind, j, tp, sibling, 4, d_recv).start()

    def relay(src, kind, j):
        side_copy(src, kind, j, across, across, 3, x_recv).wait_recv()
        side_copy(src, kind, j, across, sibling, 5, d_recv).start()

    def settle(src, kind, j):
        start, size = span(kind, j)
        both_halves(src, start, size // 2, flag(src, kind, j)).wait_recv()

    def send_all(items):
        for dst, kind, j in items:
            z_copy(me, dst, kind, j).start()

    for m in range(2):
        @pl.when(me + 1 < n)
        def _():
            w_hop(me, m, me + 1, True).start()

        @pl.when(me > 0)
        def _():
            w_hop(me, m, me - 1, True).start()

    for spot in range(n):
        @pl.when(me == spot)
        def _():
            send_all(right_plan(n, blocks, spot)[0])
            send_all(left_plan(n, blocks, spot)[0])

    small_in = [
        pltpu.make_async_copy(a, b, local.at[3 + i])
        for i, (a, b) in enumerate(
            ((query, q_in), (key_new, k_in), (value_new, v_in), (lam, lam_in), (gain, gain_in))
        )
    ]
    own_w = [
        pltpu.make_async_copy(
            mats[m],
            weights.at[pl.ds(pl.multiple_of(me * depth, depth), depth), pl.ds(m * cols, cols)],
            local.at[m],
        )
        for m in range(2)
    ]
    own_rows = pltpu.make_async_copy(prompt.at[me], rows_in.at[me], local.at[2])
    for copy in own_w + [own_rows] + small_in:
        copy.start()

    def weight_event(spot, src):
        for m in range(2):
            if src < spot:
                w_hop(src, m, me, False).wait_recv()
                if spot + 1 < n:
                    w_hop(src, m, me + 1, False).start()
            else:
                w_hop(src, m, me, False).wait_recv()
                if spot > 0:
                    w_hop(src, m, me - 1, False).start()
            w_side(src, m, grp).start()

    plans = [arrivals(n, blocks, spot) for spot in range(n)]
    aheads = [sum(kind == "big" for kind, _, _ in first) for first, _ in plans]
    orders = [
        [(s, j) for kind, s, j in first if kind == "big"] + [(s, j) for _, s, j in rest]
        for first, rest in plans
    ]
    total = len(orders[0])
    for spot in range(n):
        first = plans[spot][0]
        bigs = []

        @pl.when(me == spot)
        def _():
            lefts = [s for kind, s, _ in first if kind == "w" and s < spot]
            rights = [s for kind, s, _ in first if kind == "w" and s > spot]
            for kind, s, j in first:
                if kind == "w":
                    weight_event(spot, s)
                    if s < spot:
                        lefts.remove(s)
                        if not lefts:
                            send_all(right_plan(n, blocks, spot)[1][:HOLD])
                    else:
                        rights.remove(s)
                        if not rights:
                            send_all(left_plan(n, blocks, spot)[1][:HOLD])
                    continue
                take(s, kind, j)
                if kind == "big":
                    bigs.append((s, j))
                    if len(bigs) > 1:
                        relay(bigs[-2][0], "big", bigs[-2][1])
            if any(kind == "tail" for kind, _, _ in first):
                relay(critical(n, spot), "tail", 0)
            if spot > 0:
                send_all(left_plan(n, blocks, spot)[1][HOLD if spot < n - 1 else 0:])
            if spot < n - 1:
                send_all(right_plan(n, blocks, spot)[1][HOLD if spot > 0 else 0:])

    for copy in small_in:
        copy.wait()

    def mine(ref):
        whole = ref[...].astype(jnp.float32)
        here = lax.broadcasted_iota(jnp.int32, whole.shape, 0) == me
        return jnp.sum(jnp.where(here, whole, 0.0), axis=0, keepdims=True)

    scale = HALF ** (-0.5)
    shape = (2 * heads, cols)
    row = lax.broadcasted_iota(jnp.int32, shape, 0)
    group = lax.broadcasted_iota(jnp.int32, shape, 1) // HALF
    chosen = jnp.where(row < heads, 2 * row, 2 * (row - heads) + 1) == group
    q_mat = jnp.where(chosen, jnp.broadcast_to(mine(q_in), shape), 0.0)
    fresh = jnp.sum(q_mat * mine(k_in), axis=1, keepdims=True) * scale
    q_low[...] = q_mat.astype(jnp.bfloat16)
    spread = (heads, heads)
    mix = jnp.sum(
        jnp.where(
            lax.broadcasted_iota(jnp.int32, spread, 0) == lax.broadcasted_iota(jnp.int32, spread, 1),
            jnp.broadcast_to(lam_in[...], spread), 0.0,
        ),
        axis=1, keepdims=True,
    )

    def project_rows(src, start, size):
        both = jnp.dot(
            rows_in[src, pl.ds(start, size), :], weights[...], preferred_element_type=jnp.float32
        ).astype(jnp.bfloat16)
        at = pl.ds(pl.multiple_of(src * piece + start, BIG), size)
        keys[at, :] = both[:, :cols]
        values[at, :] = both[:, cols:]

    def score_rows(src, start, size):
        at = pl.multiple_of(src * piece + start, BIG)
        scores[:, pl.ds(at, size)] = lax.dot_general(
            q_low[...], keys[pl.ds(at, size), :], (((1,), (1,)), ((), ())),
            preferred_element_type=jnp.float32,
        ) * scale

    def compute(src, j):
        start = pl.multiple_of(j * BIG, BIG)
        project_rows(src, start, BIG)
        score_rows(src, start, BIG)

    picks = [by_spot([o[at][0] * blocks + o[at][1] for o in orders]) for at in range(total)]

    def order(k):
        pick = picks[0]
        for at in range(1, total):
            pick = jnp.where(k == at, picks[at], pick)
        return pick // blocks, lax.rem(pick, blocks)

    ahead = by_spot(aheads)

    def step(k, carry):
        src, j = order(k)
        take_big(src, j)
        src, j = order(k - 1)
        relay_big(src, j)

        @pl.when(k == ahead + START)
        def _():
            w_all(n - 1).wait_recv()
            for copy in own_w:
                copy.wait()
            own_rows.wait()

        b = k - ahead - START

        @pl.when((b >= 0) & (b < blocks + ahead))
        def _():
            src, j = order(b - blocks)
            foreign = b >= blocks

            @pl.when(foreign)
            def _():
                settle_big(src, j)

            compute(jnp.where(foreign, src, me), jnp.where(foreign, j, b))

        @pl.when(k - 2 >= ahead)
        def _():
            src, j = order(k - 2)
            settle_big(src, j)
            compute(src, j)

        return carry

    def dyn(j, q):
        quarter = BIG // 4
        return pl.ds(pl.multiple_of(j * BIG + q * quarter, quarter), quarter)

    def z_big(src, dst, j):
        return pltpu.make_async_remote_copy(
            src_ref=prompt.at[dst, dyn(j, tp)], dst_ref=rows_in.at[src, dyn(j, tp)],
            send_sem=sent.at[2], recv_sem=z_recv.at[src * blocks + j],
            device_id={"sp": dst}, device_id_type=MESH,
        )

    def side_big(src, j, q, to, send, recv):
        return pltpu.make_async_remote_copy(
            src_ref=rows_in.at[src, dyn(j, q)], dst_ref=rows_in.at[src, dyn(j, q)],
            send_sem=sent.at[send], recv_sem=recv.at[src * blocks + j],
            device_id={"tp": to}, device_id_type=MESH,
        )

    def take_big(src, j):
        z_big(src, me, j).wait_recv()
        side_big(src, j, tp, across, 3, x_recv).start()
        side_big(src, j, tp, sibling, 4, d_recv).start()

    def relay_big(src, j):
        side_big(src, j, across, across, 3, x_recv).wait_recv()
        side_big(src, j, across, sibling, 5, d_recv).start()

    def settle_big(src, j):
        both_halves(src, j * BIG, BIG // 2, src * blocks + j).wait_recv()

    lax.fori_loop(ahead, total, step, 0)

    late_fill = (me == 0) | (me == n - 1)

    @pl.when(late_fill)
    def _():
        take(crit, "tail", 0)

    src, j = order(total - 1)
    relay_big(src, j)

    def last_bigs(k, carry):
        src, j = order(k)

        @pl.when(k < total)
        def _():
            settle_big(src, j)

        @pl.when(k == total - 1)
        def _():
            take(crit, "tail", 1)

            @pl.when(late_fill)
            def _():
                relay(crit, "tail", 0)

        @pl.when(k == total)
        def _():
            take(crit, "tail", 2)
            relay(crit, "tail", 1)
            take(crit, "tail", 3)
            settle(crit, "tail", 0)
            settle(crit, "tail", 1)

        @pl.when(k == total + 1)
        def _():
            take(crit, "tail", 4)
            relay(crit, "tail", 2)
            take(crit, "tail", 5)
            for piece_ in (3, 4, 5):
                relay(crit, "tail", piece_)
            for piece_ in (2, 3, 4, 5):
                settle(crit, "tail", piece_)

        final = k >= total
        compute(jnp.where(final, crit, src), jnp.where(final, blocks - 2 + k - total, j))
        return carry

    lax.fori_loop(total - 2, total + 2, last_bigs, 0)

    s = scores[...]
    top = jnp.maximum(jnp.max(s, axis=1, keepdims=True), fresh)
    e = jnp.exp(s - top)
    fresh_e = jnp.exp(fresh - top)
    sums = jnp.sum(e, axis=1, keepdims=True) + fresh_e
    w = e / sums
    fresh_w = fresh_e / sums
    mixed = (w[:heads] - mix * w[heads:]).astype(jnp.bfloat16)
    fresh_mixed = (fresh_w[:heads] - mix * fresh_w[heads:]).astype(jnp.bfloat16).astype(jnp.float32)
    o = jnp.dot(mixed, values[...], preferred_element_type=jnp.float32)
    o = o + fresh_mixed * mine(v_in)
    for h in range(heads):
        lanes = slice(h * VDIM, (h + 1) * VDIM)
        one = o[h:h + 1, lanes]
        mean = jnp.mean(one * one, axis=1, keepdims=True)
        own[:, lanes] = one * lax.rsqrt(mean + 1e-06) * gain_in[...]

    def row_copy(step_, src):
        return pltpu.make_async_remote_copy(
            src_ref=own, dst_ref=slots.at[src], send_sem=sent.at[6], recv_sem=met.at[1],
            device_id={"sp": lax.rem(me + step_, n)}, device_id_type=MESH,
        )

    for step_ in range(1, n):
        row_copy(step_, me).start()

    def all_sent(block, at):
        pltpu.make_async_remote_copy(
            src_ref=block, dst_ref=block, send_sem=sent.at[at], recv_sem=met.at[1],
            device_id={"sp": lax.rem(me + 1, n)}, device_id_type=MESH,
        ).wait_send()

    for at in range(2, 6):
        all_sent(rows_in.at[0, pl.ds(0, (n - 1) * piece // 4)], at)
    w_all(n - 1).wait_send()
    inner = (me > 0) & (me + 1 < n)

    @pl.when(inner)
    def _():
        all_sent(weights.at[pl.ds(0, (n + 1) * half)], 0)

    @pl.when(jnp.logical_not(inner))
    def _():
        all_sent(weights.at[pl.ds(0, half)], 0)

    others = slots.at[pl.ds(0, n - 1)]
    pltpu.make_async_remote_copy(
        src_ref=others, dst_ref=others, send_sem=sent.at[6], recv_sem=met.at[1],
        device_id={"sp": lax.rem(me + 1, n)}, device_id_type=MESH,
    ).wait_recv()
    mine_row = own[...]
    for src in range(n):
        read[src:src + 1, :] = jnp.where(me == src, mine_row, slots[src]).astype(jnp.bfloat16)
    all_sent(others, 6)


def gather_project(n, prompt, w_key, w_value, query, key_new, value_new, mix_lambda, head_gain):
    count, piece, width = prompt.shape
    depth, cols = w_key.shape
    heads = mix_lambda.shape[0]
    dma = pltpu.SemaphoreType.DMA
    steps = n * (piece // BIG) + len(TAIL) - 2
    out = pltpu.VMEM((n * piece, cols), jnp.bfloat16)
    vmem = pl.BlockSpec(memory_space=pltpu.VMEM)
    hbm = pl.BlockSpec(memory_space=pltpu.HBM)
    f32, bf16 = jnp.float32, jnp.bfloat16
    return pl.pallas_call(
        functools.partial(gather_kernel, (n, piece)),
        out_shape=(out, out, pltpu.VMEM((n, cols), bf16)),
        in_specs=[hbm] * 8,
        out_specs=(vmem, vmem, vmem),
        scratch_shapes=[
            pltpu.VMEM((n, piece, width), bf16),
            pltpu.VMEM((n * depth, 2 * cols), bf16),
            pltpu.VMEM((2 * heads, n * piece), f32),
            pltpu.VMEM((2 * heads, cols), bf16),
            pltpu.VMEM((1, cols), f32),
            pltpu.VMEM((n, 1, cols), f32),
            pltpu.VMEM(query.shape, bf16),
            pltpu.VMEM(key_new.shape, bf16),
            pltpu.VMEM(value_new.shape, bf16),
            pltpu.VMEM((1, heads), f32),
            pltpu.VMEM((1, VDIM), f32),
        ]
        + [dma((steps,))] * 3
        + [dma((2 * n,)), dma((7,)), dma((2,)), dma((8,))],
        compiler_params=pltpu.CompilerParams(
            collective_id=0, has_side_effects=True,
            vmem_limit_bytes=2**26 - 2**18 - 4 * n * piece * cols,
        ),
    )(
        prompt, w_key, w_value, query, key_new, value_new,
        mix_lambda[None, :], head_gain[None, :],
    )


def write_kernel(cuts, *refs):
    ins, outs, sem = refs[:3], refs[3:6], refs[6]
    copies = []
    for i in range(2):
        size = ins[i].shape[0] // cuts
        for c in range(cuts):
            at = pl.ds(c * size, size)
            copies.append((ins[i].at[at], outs[i].at[at]))
    copies.append((ins[2], outs[2]))
    copies = [pltpu.make_async_copy(a, b, sem.at[i]) for i, (a, b) in enumerate(copies)]
    for copy in copies:
        copy.start()
    for copy in copies:
        copy.wait()


def write_out(keys, values, read):
    cuts = 4
    hbm = pl.BlockSpec(memory_space=pltpu.HBM)
    vmem = pl.BlockSpec(memory_space=pltpu.VMEM)
    return pl.pallas_call(
        functools.partial(write_kernel, cuts),
        out_shape=tuple(jax.ShapeDtypeStruct(a.shape, a.dtype) for a in (keys, values, read)),
        in_specs=[vmem] * 3,
        out_specs=(hbm, hbm, hbm),
        scratch_shapes=[pltpu.SemaphoreType.DMA((2 * cuts + 1,))],
        compiler_params=pltpu.CompilerParams(vmem_limit_bytes=2**20),
    )(keys, values, read)


def fast_body(prompt, w_key, w_value, query_new, key_new, value_new, mix_lambda, head_gain):
    count, piece, width = prompt.shape
    n = lax.axis_size("sp")
    keys, values, read = write_out(
        *gather_project(
            n, prompt, w_key, w_value, query_new, key_new, value_new, mix_lambda, head_gain
        )
    )
    cols = keys.shape[-1]
    return (keys.reshape(1, n, piece, cols), values.reshape(1, n, piece, cols), read)


def choose(mesh):
    def run(prompt, *rest):
        sizes = dict(mesh.shape)
        count, piece, width = prompt.shape
        rows = rest[0].shape[0]
        fits = (
            sizes["grp"] == 2
            and sizes["tp"] == 4
            and sizes["sp"] == count
            and count == 4
            and piece % BIG == 0
            and piece >= 6 * BIG
            and rows % 32 == 0
            and count * piece * width * 2 <= 2**25
        )
        return (fast_body if fits else body)(prompt, *rest)

    return run


def solution(mesh):
    placed = (
        P("grp", "sp", None),
        P("sp", "tp"),
        P("sp", "tp"),
        P("grp", "tp"),
        P("grp", "tp"),
        P("grp", "tp"),
        P("tp"),
        P(),
    )
    return jax.shard_map(
        choose(mesh),
        mesh=mesh,
        in_specs=placed,
        out_specs=(
            P(("grp", "sp"), None, None, "tp"),
            P(("grp", "sp"), None, None, "tp"),
            P("grp", "tp"),
        ),
        check_vma=False,
    )
```

```python
import functools

import jax
import jax.numpy as jnp
from jax import lax
from jax.experimental import pallas as pl
from jax.experimental.pallas import tpu as pltpu
from jax.sharding import PartitionSpec as P

HALF = 64
VDIM = 128
MESH = pl.DeviceIdType.MESH
BIG = 256
TAIL = (128, 128, 128, 64, 32, 32)
START = 2
HOLD = 3


def combined_all(part, axis, combine):
    gathered = jax.tree.map(lambda a: lax.all_gather(a, axis), part)

    def take(source):
        return jax.tree.map(lambda a: lax.dynamic_index_in_dim(a, source, 0, False), gathered)

    return lax.fori_loop(
        1, lax.axis_size(axis), lambda source, state: combine(state, take(source)), take(0)
    )


def project(rows, w_key, w_value):
    keys = jnp.dot(
        rows, lax.all_gather(w_key, "sp", axis=0, tiled=True), preferred_element_type=jnp.float32
    )
    values = jnp.dot(
        rows, lax.all_gather(w_value, "sp", axis=0, tiled=True), preferred_element_type=jnp.float32
    )
    return (keys.astype(jnp.bfloat16), values.astype(jnp.bfloat16))


def score_maps(query, keys):
    count, span = (keys.shape[0], keys.shape[1])
    heads = query.shape[1] // (2 * HALF)
    q_parts = query.reshape(count, heads, 2, HALF)
    k_parts = keys.reshape(count, span, heads, 2, HALF)
    return jnp.einsum(
        "shmc,slhmc->shml", q_parts, k_parts, preferred_element_type=jnp.float32
    ) * HALF ** (-0.5)


def own_scores(query, fresh_key):
    count = query.shape[0]
    heads = query.shape[1] // (2 * HALF)
    q_parts = query.astype(jnp.float32).reshape(count, heads, 2, HALF)
    k_parts = fresh_key.astype(jnp.float32).reshape(count, heads, 2, HALF)
    return jnp.sum(q_parts * k_parts, axis=-1) * HALF ** (-0.5)


def finish(reads, head_gain):
    mean = jnp.mean(reads * reads, axis=-1, keepdims=True)
    normed = reads * lax.rsqrt(mean + 1e-06) * head_gain
    return normed.reshape(reads.shape[0], -1).astype(jnp.bfloat16)


def join_totals(first, second):
    top = jnp.maximum(first[0], second[0])
    return (top, first[1] * jnp.exp(first[0] - top) + second[1] * jnp.exp(second[0] - top))


def placed(part_rows, prompts, first, fill):
    base = jnp.full((prompts,) + part_rows.shape[1:], fill, jnp.float32)
    return lax.dynamic_update_slice_in_dim(base, part_rows, first, 0)


def cache_read(query_new, key_new, value_new, keys, values, mix_lambda, head_gain, first):
    count, span = (keys.shape[0], keys.shape[1])
    prompts = query_new.shape[0]
    heads = mix_lambda.shape[0]
    query = lax.dynamic_slice_in_dim(query_new, first, count, 0)
    scores = score_maps(query, keys)
    fresh_all = own_scores(query_new, key_new)
    fresh = lax.dynamic_slice_in_dim(fresh_all, first, count, 0)
    local_top = jnp.maximum(jnp.max(scores, axis=-1), fresh)
    local_total = jnp.sum(jnp.exp(scores - local_top[..., None]), axis=-1)
    top_all, cache_total = combined_all(
        (placed(local_top, prompts, first, -1e30), placed(local_total, prompts, first, 0.0)),
        "sp",
        join_totals,
    )
    own = jnp.exp(fresh_all - top_all)
    total_all = cache_total + own
    top = lax.dynamic_slice_in_dim(top_all, first, count, 0)
    total = lax.dynamic_slice_in_dim(total_all, first, count, 0)
    probs = jnp.exp(scores - top[..., None]) / total[..., None]
    mixed = (probs[:, :, 0] - mix_lambda[None, :, None] * probs[:, :, 1]).astype(jnp.bfloat16)
    value_parts = values.reshape(count, span, heads, VDIM)
    partial_value = jnp.einsum(
        "shl,slhv->shv", mixed, value_parts, preferred_element_type=jnp.float32
    )
    reads = lax.psum(placed(partial_value, prompts, first, 0.0), "sp")
    own_prob = own / total_all
    own_mixed = (own_prob[:, :, 0] - mix_lambda[None, :] * own_prob[:, :, 1]).astype(jnp.bfloat16)
    reads = reads + own_mixed.astype(jnp.float32)[..., None] * value_new.astype(
        jnp.float32
    ).reshape(prompts, heads, VDIM)
    return finish(reads, head_gain)


def block_read(
    query_new, key_new, value_new, key_cache, value_cache, mix_lambda, head_gain, spread
):
    blocks, sub = (key_cache.shape[1], key_cache.shape[2])
    first = lax.axis_index("sp") // spread
    keys = key_cache.reshape(1, blocks * sub, -1)
    values = value_cache.reshape(1, blocks * sub, -1)
    return cache_read(query_new, key_new, value_new, keys, values, mix_lambda, head_gain, first)


def body(prompt, w_key, w_value, query_new, key_new, value_new, mix_lambda, head_gain):
    count, piece, width = prompt.shape
    spread = lax.axis_size("sp") // count
    sub = piece // spread
    keys, values = project(prompt.reshape(count * piece, width), w_key, w_value)
    key_blocks = keys.reshape(count * spread, 1, sub, -1)
    value_blocks = values.reshape(count * spread, 1, sub, -1)
    key_cache, value_cache = (
        lax.all_to_all(key_blocks, "sp", split_axis=0, concat_axis=1, tiled=True),
        lax.all_to_all(value_blocks, "sp", split_axis=0, concat_axis=1, tiled=True),
    )
    first_read = block_read(
        query_new, key_new, value_new, key_cache, value_cache, mix_lambda, head_gain, spread
    )
    return (key_cache, value_cache, first_read)


def critical(n, spot):
    return n // 2 - 1 if spot >= n // 2 else n // 2


def tail_pieces(blocks):
    return [("big", j) for j in range(blocks - 2)] + [("tail", j) for j in range(len(TAIL))]


def right_plan(n, blocks, src):
    far, near = n - 1, n // 2
    every = [("big", j) for j in range(blocks)]
    if src == 0:
        return [(1, *p) for p in every], [(d, *p) for p in every for d in (far, near)]
    if src == near:
        return [(far, *p) for p in every[:1]], [(far, *p) for p in every[1:]]
    if src == far:
        return [], []
    to_near = [(near, *p) for p in tail_pieces(blocks)]
    to_far = [(far, *p) for p in tail_pieces(blocks)]
    fill = blocks - 2
    early = [to_near.pop(fill)]
    late = to_near[:3] + to_far[:2] + to_near[3:4] + to_far[2:fill + 1]
    rest = zip(to_far[fill + 1:], to_near[4:])
    return early, late + [item for pair in rest for item in pair]


def left_plan(n, blocks, src):
    early, late = right_plan(n, blocks, n - 1 - src)
    flip = lambda items: [(n - 1 - dst, kind, j) for dst, kind, j in items]
    return flip(early), flip(late)


def arrivals(n, blocks, spot):
    if spot < n // 2:
        first, rest = arrivals(n, blocks, n - 1 - spot)
        flip = lambda items: [(kind, n - 1 - src, j) for kind, src, j in items]
        return flip(first), flip(rest)
    far = n - 1
    crit = [("big", 1, j) for j in range(blocks - 2)]
    through = [("big", 0, j) for j in range(blocks)]
    if spot == far:
        near = [("big", 2, j) for j in range(blocks)]
        first = [("w", 2, 0), near[0], ("w", 1, 0), ("w", 0, 0)]
        rest = [item for pair in zip(near[1:], through) for item in pair]
        return first, rest + through[blocks - 1:] + crit
    near = [("big", 3, j) for j in range(blocks)]
    first = [("w", 1, 0), ("w", 3, 0), ("tail", 1, 0), near[0], near[1], ("w", 0, 0)]
    rest = [near[2], crit[0], near[3], crit[1], near[4], crit[2], near[5]]
    return first, rest + near[6:] + through + crit[3:]


def gather_kernel(
    plan, prompt, w_key, w_value, query, key_new, value_new, lam, gain,
    keys, values, read,
    rows_in, weights, scores, q_low, own, slots,
    new_in, lam_in, gain_in,
    z_recv, x_recv, d_recv, w_recv, sent, met, local,
):
    n, piece = plan
    blocks = piece // BIG
    me = lax.axis_index("sp")
    tp = lax.axis_index("tp")
    grp = lax.axis_index("grp")
    across = lax.rem(tp + 2, 4)
    sibling = tp + 1 - 2 * lax.rem(tp, 2)
    far = lax.rem(sibling + 2, 4)
    depth, cols = w_key.shape
    heads = cols // VDIM
    half = depth // 2
    mats = (w_key, w_value)

    def by_spot(values_):
        pick = values_[0]
        for spot in range(1, n):
            pick = jnp.where(me == spot, values_[spot], pick)
        return pick

    crit = by_spot([critical(n, spot) for spot in range(n)])

    def span(kind, j):
        if kind == "big":
            return j * BIG, BIG
        return piece - sum(TAIL[j:]), TAIL[j]

    def big_flag(src, dst, j):
        return lax.rem(src - dst - 1 + n, n) * blocks + j

    def flag(src, dst, kind, j):
        if kind == "big":
            return big_flag(src, dst, j)
        return big_flag(src, dst, blocks - 2 + j) if j < 2 else (n - 1) * blocks + j - 2

    def part(kind, j, q):
        start, size = span(kind, j)
        quarter = size // 4
        return pl.ds(pl.multiple_of(start + q * quarter, quarter), quarter)

    mine_w = pl.ds(pl.multiple_of(me * depth, depth), depth)
    for m in range(2):
        pltpu.make_async_copy(
            mats[m], weights.at[mine_w, pl.ds(m * cols, cols)], local.at[0]
        ).start()

    barrier = pltpu.get_barrier_semaphore()

    @pl.when(me + 1 < n)
    def _():
        pl.semaphore_signal(barrier, inc=1, device_id={"sp": me + 1}, device_id_type=MESH)

    @pl.when(me > 0)
    def _():
        pl.semaphore_signal(barrier, inc=1, device_id={"sp": me - 1}, device_id_type=MESH)

    pl.semaphore_signal(barrier, inc=1, device_id={"tp": across}, device_id_type=MESH)
    pl.semaphore_signal(barrier, inc=1, device_id={"tp": sibling}, device_id_type=MESH)
    pl.semaphore_signal(barrier, inc=1, device_id={"grp": 1 - grp}, device_id_type=MESH)
    pl.semaphore_wait(barrier, jnp.where((me > 0) & (me + 1 < n), 5, 4))
    pltpu.make_async_copy(weights.at[mine_w], weights.at[mine_w], local.at[0]).wait()

    def w_slot(src, m, g):
        return weights.at[pl.ds(pl.multiple_of(src * depth + g * half, half), half),
                          pl.ds(m * cols, cols)]

    def w_hop(src, m, to):
        return pltpu.make_async_remote_copy(
            src_ref=w_slot(src, m, grp), dst_ref=w_slot(src, m, grp),
            send_sem=sent.at[0], recv_sem=w_recv.at[src * 2 + m],
            device_id={"sp": to}, device_id_type=MESH,
        )

    def w_side(src, m, g):
        return pltpu.make_async_remote_copy(
            src_ref=w_slot(src, m, g), dst_ref=w_slot(src, m, g),
            send_sem=sent.at[0], recv_sem=met.at[0],
            device_id={"grp": 1 - grp}, device_id_type=MESH,
        )

    def w_all(count):
        block = weights.at[pl.ds(0, count * half)]
        return pltpu.make_async_remote_copy(
            src_ref=block, dst_ref=block, send_sem=sent.at[1], recv_sem=met.at[0],
            device_id={"grp": 1 - grp}, device_id_type=MESH,
        )

    def z_copy(src, dst, kind, j):
        return pltpu.make_async_remote_copy(
            src_ref=prompt.at[dst, part(kind, j, tp)], dst_ref=rows_in.at[src, part(kind, j, tp)],
            send_sem=sent.at[1], recv_sem=z_recv.at[flag(src, dst, kind, j)],
            device_id={"sp": dst}, device_id_type=MESH,
        )

    def side_copy(src, kind, j, q, to, recv):
        return pltpu.make_async_remote_copy(
            src_ref=rows_in.at[src, part(kind, j, q)], dst_ref=rows_in.at[src, part(kind, j, q)],
            send_sem=sent.at[1], recv_sem=recv.at[flag(src, me, kind, j)],
            device_id={"tp": to}, device_id_type=MESH,
        )

    def both_halves(src, start, size, at):
        rows = rows_in.at[src, pl.ds(pl.multiple_of(start, size), size)]
        return pltpu.make_async_remote_copy(
            src_ref=rows, dst_ref=rows, send_sem=sent.at[1], recv_sem=d_recv.at[at],
            device_id={"tp": sibling}, device_id_type=MESH,
        )

    even = lax.rem(tp, 2) == 0

    def skips(kind, j):
        return kind == "tail" and j >= len(TAIL) - 2

    def take(src, kind, j):
        z_copy(src, me, kind, j).wait_recv()
        side_copy(src, kind, j, tp, across, x_recv).start()
        if skips(kind, j):
            @pl.when(even)
            def _():
                side_copy(src, kind, j, tp, far, d_recv).start()

        side_copy(src, kind, j, tp, sibling, d_recv).start()

    def relay(src, kind, j):
        side_copy(src, kind, j, across, across, x_recv).wait_recv()

        @pl.when(jnp.logical_not(even & skips(kind, j)))
        def _():
            side_copy(src, kind, j, across, sibling, d_recv).start()

    def settle(src, kind, j):
        start, size = span(kind, j)
        both_halves(src, start, size // 2, flag(src, me, kind, j)).wait_recv()

    def send_all(items):
        for dst, kind, j in items:
            z_copy(me, dst, kind, j).start()

    for m in range(2):
        @pl.when(me + 1 < n)
        def _():
            w_hop(me, m, me + 1).start()

        @pl.when(me > 0)
        def _():
            w_hop(me, m, me - 1).start()

    for spot in range(n):
        @pl.when(me == spot)
        def _():
            send_all(right_plan(n, blocks, spot)[0])
            send_all(left_plan(n, blocks, spot)[0])

    own_rows = pltpu.make_async_copy(prompt.at[me], rows_in.at[me], local.at[1])
    small_in = [
        pltpu.make_async_copy(a, b, local.at[at])
        for a, b, at in (
            (query, new_in.at[0], 2), (key_new, new_in.at[1], 2), (value_new, new_in.at[2], 2),
            (lam, lam_in, 3), (gain, gain_in, 4),
        )
    ]
    for copy in [own_rows] + small_in:
        copy.start()

    def weight_event(spot, src):
        for m in range(2):
            if src < spot:
                w_hop(src, m, me).wait_recv()
                if spot + 1 < n:
                    w_hop(src, m, me + 1).start()
            else:
                w_hop(src, m, me).wait_recv()
                if spot > 0:
                    w_hop(src, m, me - 1).start()
            w_side(src, m, grp).start()

    plans = [arrivals(n, blocks, spot) for spot in range(n)]
    aheads = [sum(kind == "big" for kind, _, _ in first) for first, _ in plans]
    orders = [
        [(s, j) for kind, s, j in first if kind == "big"] + [(s, j) for _, s, j in rest]
        for first, rest in plans
    ]
    total = len(orders[0])
    for spot in range(n):
        first = plans[spot][0]
        bigs = []

        @pl.when(me == spot)
        def _():
            lefts = [s for kind, s, _ in first if kind == "w" and s < spot]
            rights = [s for kind, s, _ in first if kind == "w" and s > spot]
            for kind, s, j in first:
                if kind == "w":
                    weight_event(spot, s)
                    if s < spot:
                        lefts.remove(s)
                        if not lefts:
                            send_all(right_plan(n, blocks, spot)[1][:HOLD])
                    else:
                        rights.remove(s)
                        if not rights:
                            send_all(left_plan(n, blocks, spot)[1][:HOLD])
                    continue
                take(s, kind, j)
                if kind == "big":
                    bigs.append((s, j))
                    if len(bigs) > 1:
                        relay(bigs[-2][0], "big", bigs[-2][1])
            if any(kind == "tail" for kind, _, _ in first):
                relay(critical(n, spot), "tail", 0)
            if spot > 0:
                send_all(left_plan(n, blocks, spot)[1][HOLD if spot < n - 1 else 0:])
            if spot < n - 1:
                send_all(right_plan(n, blocks, spot)[1][HOLD if spot > 0 else 0:])

    pltpu.make_async_copy(new_in, new_in, local.at[2]).wait()
    for copy in small_in[3:]:
        copy.wait()

    def mine(which):
        whole = new_in[which].astype(jnp.float32)
        here = lax.broadcasted_iota(jnp.int32, whole.shape, 0) == me
        return jnp.sum(jnp.where(here, whole, 0.0), axis=0, keepdims=True)

    scale = HALF ** (-0.5)
    shape = (2 * heads, cols)
    row = lax.broadcasted_iota(jnp.int32, shape, 0)
    group = lax.broadcasted_iota(jnp.int32, shape, 1) // HALF
    chosen = jnp.where(row < heads, 2 * row, 2 * (row - heads) + 1) == group
    q_mat = jnp.where(chosen, jnp.broadcast_to(mine(0), shape), 0.0)
    fresh = jnp.sum(q_mat * mine(1), axis=1, keepdims=True) * scale
    q_low[...] = q_mat.astype(jnp.bfloat16)
    spread = (heads, heads)
    mix = jnp.sum(
        jnp.where(
            lax.broadcasted_iota(jnp.int32, spread, 0) == lax.broadcasted_iota(jnp.int32, spread, 1),
            jnp.broadcast_to(lam_in[...], spread), 0.0,
        ),
        axis=1, keepdims=True,
    )

    def project_rows(src, start, size):
        both = jnp.dot(
            rows_in[src, pl.ds(start, size), :], weights[...], preferred_element_type=jnp.float32
        ).astype(jnp.bfloat16)
        at = pl.ds(pl.multiple_of(src * piece + start, BIG // 2), size)
        keys[at, :] = both[:, :cols]
        values[at, :] = both[:, cols:]

    def score_rows(src, start, size):
        at = pl.multiple_of(src * piece + start, BIG // 2)
        scores[:, pl.ds(at, size)] = lax.dot_general(
            q_low[...], keys[pl.ds(at, size), :], (((1,), (1,)), ((), ())),
            preferred_element_type=jnp.float32,
        ) * scale

    def compute(src, j):
        start = pl.multiple_of(j * BIG, BIG)
        project_rows(src, start, BIG)
        score_rows(src, start, BIG)

    picks = [by_spot([o[at][0] * blocks + o[at][1] for o in orders]) for at in range(total)]

    def order(k):
        pick = picks[0]
        for at in range(1, total):
            pick = jnp.where(k == at, picks[at], pick)
        return pick // blocks, lax.rem(pick, blocks)

    ahead = by_spot(aheads)

    def step(k, carry):
        src, j = order(k)
        take_big(src, j)
        src, j = order(k - 1)
        relay_big(src, j)

        @pl.when(k == ahead + START)
        def _():
            w_all(n - 1).wait_recv()
            own_rows.wait()

        b = k - ahead - START

        @pl.when((b >= 0) & (b < blocks + ahead))
        def _():
            src, j = order(b - blocks)
            foreign = b >= blocks

            @pl.when(foreign)
            def _():
                settle_big(src, j)

            compute(jnp.where(foreign, src, me), jnp.where(foreign, j, b))

        @pl.when(k - 2 >= ahead)
        def _():
            src, j = order(k - 2)
            settle_big(src, j)
            compute(src, j)

        return carry

    def dyn(j, q):
        quarter = BIG // 4
        return pl.ds(pl.multiple_of(j * BIG + q * quarter, quarter), quarter)

    def z_big(src, dst, j):
        return pltpu.make_async_remote_copy(
            src_ref=prompt.at[dst, dyn(j, tp)], dst_ref=rows_in.at[src, dyn(j, tp)],
            send_sem=sent.at[1], recv_sem=z_recv.at[big_flag(src, dst, j)],
            device_id={"sp": dst}, device_id_type=MESH,
        )

    def side_big(src, j, q, to, recv):
        return pltpu.make_async_remote_copy(
            src_ref=rows_in.at[src, dyn(j, q)], dst_ref=rows_in.at[src, dyn(j, q)],
            send_sem=sent.at[1], recv_sem=recv.at[big_flag(src, me, j)],
            device_id={"tp": to}, device_id_type=MESH,
        )

    def take_big(src, j):
        z_big(src, me, j).wait_recv()
        side_big(src, j, tp, across, x_recv).start()
        side_big(src, j, tp, sibling, d_recv).start()

    def relay_big(src, j):
        side_big(src, j, across, across, x_recv).wait_recv()
        side_big(src, j, across, sibling, d_recv).start()

    def settle_big(src, j):
        both_halves(src, j * BIG, BIG // 2, big_flag(src, me, j)).wait_recv()

    lax.fori_loop(ahead, total, step, 0)

    late_fill = (me == 0) | (me == n - 1)

    @pl.when(late_fill)
    def _():
        take(crit, "tail", 0)

    src, j = order(total - 1)
    relay_big(src, j)

    def last_bigs(k, carry):
        src, j = order(k)

        @pl.when(k < total)
        def _():
            settle_big(src, j)

        @pl.when(k == total - 1)
        def _():
            take(crit, "tail", 1)

            @pl.when(late_fill)
            def _():
                relay(crit, "tail", 0)

        @pl.when(k == total)
        def _():
            take(crit, "tail", 2)
            relay(crit, "tail", 1)
            for piece_ in (3, 4, 5):
                take(crit, "tail", piece_)
            relay(crit, "tail", 2)
            settle(crit, "tail", 0)
            settle(crit, "tail", 1)

        final = k == total
        compute(jnp.where(final, crit, src), jnp.where(final, blocks - 2, j))
        return carry

    lax.fori_loop(total - 2, total + 1, last_bigs, 0)

    def last_rows(i, carry):
        @pl.when(i == 0)
        def _():
            relay(crit, "tail", 3)
            settle(crit, "tail", 2)

        @pl.when((i == 0) != even)
        def _():
            for piece_ in (4, 5):
                relay(crit, "tail", piece_)

        @pl.when(i == 1)
        def _():
            for piece_ in (3, 4, 5):
                settle(crit, "tail", piece_)

        start = pl.multiple_of(piece - BIG + i * (BIG // 2), BIG // 2)
        project_rows(crit, start, BIG // 2)
        score_rows(crit, start, BIG // 2)
        return carry

    lax.fori_loop(0, 2, last_rows, 0)

    s = scores[...]
    top = jnp.maximum(jnp.max(s, axis=1, keepdims=True), fresh)
    e = jnp.exp(s - top)
    fresh_e = jnp.exp(fresh - top)
    sums = jnp.sum(e, axis=1, keepdims=True) + fresh_e
    w = e / sums
    fresh_w = fresh_e / sums
    mixed = (w[:heads] - mix * w[heads:]).astype(jnp.bfloat16)
    fresh_mixed = (fresh_w[:heads] - mix * fresh_w[heads:]).astype(jnp.bfloat16).astype(jnp.float32)
    o = jnp.dot(mixed, values[...], preferred_element_type=jnp.float32)
    o = o + fresh_mixed * mine(2)
    for h in range(heads):
        lanes = slice(h * VDIM, (h + 1) * VDIM)
        one = o[h:h + 1, lanes]
        mean = jnp.mean(one * one, axis=1, keepdims=True)
        own[:, lanes] = one * lax.rsqrt(mean + 1e-06) * gain_in[...]

    def row_copy(step_, src):
        return pltpu.make_async_remote_copy(
            src_ref=own, dst_ref=slots.at[src], send_sem=sent.at[2], recv_sem=met.at[1],
            device_id={"sp": lax.rem(me + step_, n)}, device_id_type=MESH,
        )

    for step_ in range(1, n):
        row_copy(step_, me).start()

    def all_sent(block, at):
        pltpu.make_async_remote_copy(
            src_ref=block, dst_ref=block, send_sem=sent.at[at], recv_sem=met.at[1],
            device_id={"sp": lax.rem(me + 1, n)}, device_id_type=MESH,
        ).wait_send()

    all_sent(rows_in.at[pl.ds(0, n - 1)], 1)
    inner = (me > 0) & (me + 1 < n)

    @pl.when(inner)
    def _():
        all_sent(weights.at[pl.ds(0, 2 * n * half)], 0)

    @pl.when(jnp.logical_not(inner))
    def _():
        all_sent(weights.at[pl.ds(0, n * half)], 0)

    others = slots.at[pl.ds(0, n - 1)]
    pltpu.make_async_remote_copy(
        src_ref=others, dst_ref=others, send_sem=sent.at[2], recv_sem=met.at[1],
        device_id={"sp": lax.rem(me + 1, n)}, device_id_type=MESH,
    ).wait_recv()
    mine_row = own[...]
    for src in range(n):
        read[src:src + 1, :] = jnp.where(me == src, mine_row, slots[src]).astype(jnp.bfloat16)
    all_sent(others, 2)


def gather_project(n, prompt, w_key, w_value, query, key_new, value_new, mix_lambda, head_gain):
    count, piece, width = prompt.shape
    depth, cols = w_key.shape
    heads = mix_lambda.shape[0]
    dma = pltpu.SemaphoreType.DMA
    steps = (n - 1) * (piece // BIG) + len(TAIL) - 2
    out = pltpu.VMEM((n * piece, cols), jnp.bfloat16)
    vmem = pl.BlockSpec(memory_space=pltpu.VMEM)
    hbm = pl.BlockSpec(memory_space=pltpu.HBM)
    f32, bf16 = jnp.float32, jnp.bfloat16
    return pl.pallas_call(
        functools.partial(gather_kernel, (n, piece)),
        out_shape=(out, out, pltpu.VMEM((n, cols), bf16)),
        in_specs=[hbm] * 8,
        out_specs=(vmem, vmem, vmem),
        scratch_shapes=[
            pltpu.VMEM((n, piece, width), bf16),
            pltpu.VMEM((n * depth, 2 * cols), bf16),
            pltpu.VMEM((2 * heads, n * piece), f32),
            pltpu.VMEM((2 * heads, cols), bf16),
            pltpu.VMEM((1, cols), f32),
            pltpu.VMEM((n, 1, cols), f32),
            pltpu.VMEM((3, *query.shape), bf16),
            pltpu.VMEM((1, heads), f32),
            pltpu.VMEM((1, VDIM), f32),
        ]
        + [dma((steps,))] * 3
        + [dma((2 * n,)), dma((3,)), dma((2,)), dma((5,))],
        compiler_params=pltpu.CompilerParams(
            collective_id=0, has_side_effects=True,
            vmem_limit_bytes=2**26 - 2**18 - 4 * n * piece * cols,
        ),
    )(
        prompt, w_key, w_value, query, key_new, value_new,
        mix_lambda[None, :], head_gain[None, :],
    )


def write_kernel(cuts, *refs):
    ins, outs, sem = refs[:3], refs[3:6], refs[6]
    copies = []
    for i in range(2):
        size = ins[i].shape[0] // cuts
        for c in range(cuts):
            at = pl.ds(c * size, size)
            copies.append((ins[i].at[at], outs[i].at[at]))
    copies.append((ins[2], outs[2]))
    copies = [pltpu.make_async_copy(a, b, sem.at[i]) for i, (a, b) in enumerate(copies)]
    for copy in copies:
        copy.start()
    for copy in copies:
        copy.wait()


def write_out(keys, values, read):
    cuts = 4
    hbm = pl.BlockSpec(memory_space=pltpu.HBM)
    vmem = pl.BlockSpec(memory_space=pltpu.VMEM)
    return pl.pallas_call(
        functools.partial(write_kernel, cuts),
        out_shape=tuple(jax.ShapeDtypeStruct(a.shape, a.dtype) for a in (keys, values, read)),
        in_specs=[vmem] * 3,
        out_specs=(hbm, hbm, hbm),
        scratch_shapes=[pltpu.SemaphoreType.DMA((2 * cuts + 1,))],
        compiler_params=pltpu.CompilerParams(vmem_limit_bytes=2**20),
    )(keys, values, read)


def fast_body(prompt, w_key, w_value, query_new, key_new, value_new, mix_lambda, head_gain):
    count, piece, width = prompt.shape
    n = lax.axis_size("sp")
    keys, values, read = write_out(
        *gather_project(
            n, prompt, w_key, w_value, query_new, key_new, value_new, mix_lambda, head_gain
        )
    )
    cols = keys.shape[-1]
    return (keys.reshape(1, n, piece, cols), values.reshape(1, n, piece, cols), read)


def choose(mesh):
    def run(prompt, *rest):
        sizes = dict(mesh.shape)
        count, piece, width = prompt.shape
        rows = rest[0].shape[0]
        fits = (
            sizes["grp"] == 2
            and sizes["tp"] == 4
            and sizes["sp"] == count
            and count == 4
            and piece % BIG == 0
            and piece >= 6 * BIG
            and rows % 32 == 0
            and count * piece * width * 2 <= 2**25
        )
        return (fast_body if fits else body)(prompt, *rest)

    return run


def solution(mesh):
    placed = (
        P("grp", "sp", None),
        P("sp", "tp"),
        P("sp", "tp"),
        P("grp", "tp"),
        P("grp", "tp"),
        P("grp", "tp"),
        P("tp"),
        P(),
    )
    return jax.shard_map(
        choose(mesh),
        mesh=mesh,
        in_specs=placed,
        out_specs=(
            P(("grp", "sp"), None, None, "tp"),
            P(("grp", "sp"), None, None, "tp"),
            P("grp", "tp"),
        ),
        check_vma=False,
    )
```

```python
import functools

import jax
import jax.numpy as jnp
from jax import lax
from jax.experimental import pallas as pl
from jax.experimental.pallas import tpu as pltpu
from jax.sharding import PartitionSpec as P

HALF = 64
VDIM = 128
MESH = pl.DeviceIdType.MESH
BIG = 256
TAIL = (128, 128, 128, 64, 32, 32)
START = 2
HOLD = 3


def combined_all(part, axis, combine):
    gathered = jax.tree.map(lambda a: lax.all_gather(a, axis), part)

    def take(source):
        return jax.tree.map(lambda a: lax.dynamic_index_in_dim(a, source, 0, False), gathered)

    return lax.fori_loop(
        1, lax.axis_size(axis), lambda source, state: combine(state, take(source)), take(0)
    )


def project(rows, w_key, w_value):
    keys = jnp.dot(
        rows, lax.all_gather(w_key, "sp", axis=0, tiled=True), preferred_element_type=jnp.float32
    )
    values = jnp.dot(
        rows, lax.all_gather(w_value, "sp", axis=0, tiled=True), preferred_element_type=jnp.float32
    )
    return (keys.astype(jnp.bfloat16), values.astype(jnp.bfloat16))


def score_maps(query, keys):
    count, span = (keys.shape[0], keys.shape[1])
    heads = query.shape[1] // (2 * HALF)
    q_parts = query.reshape(count, heads, 2, HALF)
    k_parts = keys.reshape(count, span, heads, 2, HALF)
    return jnp.einsum(
        "shmc,slhmc->shml", q_parts, k_parts, preferred_element_type=jnp.float32
    ) * HALF ** (-0.5)


def own_scores(query, fresh_key):
    count = query.shape[0]
    heads = query.shape[1] // (2 * HALF)
    q_parts = query.astype(jnp.float32).reshape(count, heads, 2, HALF)
    k_parts = fresh_key.astype(jnp.float32).reshape(count, heads, 2, HALF)
    return jnp.sum(q_parts * k_parts, axis=-1) * HALF ** (-0.5)


def finish(reads, head_gain):
    mean = jnp.mean(reads * reads, axis=-1, keepdims=True)
    normed = reads * lax.rsqrt(mean + 1e-06) * head_gain
    return normed.reshape(reads.shape[0], -1).astype(jnp.bfloat16)


def join_totals(first, second):
    top = jnp.maximum(first[0], second[0])
    return (top, first[1] * jnp.exp(first[0] - top) + second[1] * jnp.exp(second[0] - top))


def placed(part_rows, prompts, first, fill):
    base = jnp.full((prompts,) + part_rows.shape[1:], fill, jnp.float32)
    return lax.dynamic_update_slice_in_dim(base, part_rows, first, 0)


def cache_read(query_new, key_new, value_new, keys, values, mix_lambda, head_gain, first):
    count, span = (keys.shape[0], keys.shape[1])
    prompts = query_new.shape[0]
    heads = mix_lambda.shape[0]
    query = lax.dynamic_slice_in_dim(query_new, first, count, 0)
    scores = score_maps(query, keys)
    fresh_all = own_scores(query_new, key_new)
    fresh = lax.dynamic_slice_in_dim(fresh_all, first, count, 0)
    local_top = jnp.maximum(jnp.max(scores, axis=-1), fresh)
    local_total = jnp.sum(jnp.exp(scores - local_top[..., None]), axis=-1)
    top_all, cache_total = combined_all(
        (placed(local_top, prompts, first, -1e30), placed(local_total, prompts, first, 0.0)),
        "sp",
        join_totals,
    )
    own = jnp.exp(fresh_all - top_all)
    total_all = cache_total + own
    top = lax.dynamic_slice_in_dim(top_all, first, count, 0)
    total = lax.dynamic_slice_in_dim(total_all, first, count, 0)
    probs = jnp.exp(scores - top[..., None]) / total[..., None]
    mixed = (probs[:, :, 0] - mix_lambda[None, :, None] * probs[:, :, 1]).astype(jnp.bfloat16)
    value_parts = values.reshape(count, span, heads, VDIM)
    partial_value = jnp.einsum(
        "shl,slhv->shv", mixed, value_parts, preferred_element_type=jnp.float32
    )
    reads = lax.psum(placed(partial_value, prompts, first, 0.0), "sp")
    own_prob = own / total_all
    own_mixed = (own_prob[:, :, 0] - mix_lambda[None, :] * own_prob[:, :, 1]).astype(jnp.bfloat16)
    reads = reads + own_mixed.astype(jnp.float32)[..., None] * value_new.astype(
        jnp.float32
    ).reshape(prompts, heads, VDIM)
    return finish(reads, head_gain)


def block_read(
    query_new, key_new, value_new, key_cache, value_cache, mix_lambda, head_gain, spread
):
    blocks, sub = (key_cache.shape[1], key_cache.shape[2])
    first = lax.axis_index("sp") // spread
    keys = key_cache.reshape(1, blocks * sub, -1)
    values = value_cache.reshape(1, blocks * sub, -1)
    return cache_read(query_new, key_new, value_new, keys, values, mix_lambda, head_gain, first)


def body(prompt, w_key, w_value, query_new, key_new, value_new, mix_lambda, head_gain):
    count, piece, width = prompt.shape
    spread = lax.axis_size("sp") // count
    sub = piece // spread
    keys, values = project(prompt.reshape(count * piece, width), w_key, w_value)
    key_blocks = keys.reshape(count * spread, 1, sub, -1)
    value_blocks = values.reshape(count * spread, 1, sub, -1)
    key_cache, value_cache = (
        lax.all_to_all(key_blocks, "sp", split_axis=0, concat_axis=1, tiled=True),
        lax.all_to_all(value_blocks, "sp", split_axis=0, concat_axis=1, tiled=True),
    )
    first_read = block_read(
        query_new, key_new, value_new, key_cache, value_cache, mix_lambda, head_gain, spread
    )
    return (key_cache, value_cache, first_read)


def critical(n, spot):
    return n // 2 - 1 if spot >= n // 2 else n // 2


def tail_pieces(blocks):
    return [("big", j) for j in range(blocks - 2)] + [("tail", j) for j in range(len(TAIL))]


def right_plan(n, blocks, src):
    far, near = n - 1, n // 2
    every = [("big", j) for j in range(blocks)]
    if src == 0:
        return [(1, *p) for p in every], [(d, *p) for p in every for d in (far, near)]
    if src == near:
        return [(far, *p) for p in every[:1]], [(far, *p) for p in every[1:]]
    if src == far:
        return [], []
    to_near = [(near, *p) for p in tail_pieces(blocks)]
    to_far = [(far, *p) for p in tail_pieces(blocks)]
    fill = blocks - 2
    early = [to_near.pop(fill)]
    late = to_near[:3] + to_far[:2] + to_near[3:4] + to_far[2:fill + 1]
    rest = zip(to_far[fill + 1:], to_near[4:])
    return early, late + [item for pair in rest for item in pair]


def left_plan(n, blocks, src):
    early, late = right_plan(n, blocks, n - 1 - src)
    flip = lambda items: [(n - 1 - dst, kind, j) for dst, kind, j in items]
    return flip(early), flip(late)


def arrivals(n, blocks, spot):
    if spot < n // 2:
        first, rest = arrivals(n, blocks, n - 1 - spot)
        flip = lambda items: [(kind, n - 1 - src, j) for kind, src, j in items]
        return flip(first), flip(rest)
    far = n - 1
    crit = [("big", 1, j) for j in range(blocks - 2)]
    through = [("big", 0, j) for j in range(blocks)]
    if spot == far:
        near = [("big", 2, j) for j in range(blocks)]
        first = [("w", 2, 0), near[0], ("w", 1, 0), ("w", 0, 0)]
        rest = [item for pair in zip(near[1:], through) for item in pair]
        return first, rest + through[blocks - 1:] + crit
    near = [("big", 3, j) for j in range(blocks)]
    first = [("w", 1, 0), ("w", 3, 0), ("tail", 1, 0), near[0], near[1], ("w", 0, 0)]
    rest = [near[2], crit[0], near[3], crit[1], near[4], crit[2], near[5]]
    return first, rest + near[6:] + through + crit[3:]


def gather_kernel(
    plan, prompt, w_key, w_value, query, key_new, value_new, lam, gain,
    keys, values, read,
    rows_in, weights, scores, q_low, own, slots,
    new_in, lam_in, gain_in,
    z_recv, x_recv, d_recv, w_recv, sent, met, local,
):
    n, piece = plan
    blocks = piece // BIG
    me = lax.axis_index("sp")
    tp = lax.axis_index("tp")
    grp = lax.axis_index("grp")
    across = lax.rem(tp + 2, 4)
    sibling = tp + 1 - 2 * lax.rem(tp, 2)
    far = lax.rem(sibling + 2, 4)
    depth, cols = w_key.shape
    heads = cols // VDIM
    half = depth // 2
    mats = (w_key, w_value)

    def by_spot(values_):
        pick = values_[0]
        for spot in range(1, n):
            pick = jnp.where(me == spot, values_[spot], pick)
        return pick

    crit = by_spot([critical(n, spot) for spot in range(n)])

    def span(kind, j):
        if kind == "big":
            return j * BIG, BIG
        return piece - sum(TAIL[j:]), TAIL[j]

    def big_flag(src, dst, j):
        return lax.rem(src - dst - 1 + n, n) * blocks + j

    def flag(src, dst, kind, j):
        if kind == "big":
            return big_flag(src, dst, j)
        return big_flag(src, dst, blocks - 2 + j) if j < 2 else (n - 1) * blocks + j - 2

    def part(kind, j, q):
        start, size = span(kind, j)
        quarter = size // 4
        return pl.ds(pl.multiple_of(start + q * quarter, quarter), quarter)

    mine_w = pl.ds(pl.multiple_of(me * depth, depth), depth)
    for m in range(2):
        pltpu.make_async_copy(
            mats[m], weights.at[mine_w, pl.ds(m * cols, cols)], local.at[0]
        ).start()

    barrier = pltpu.get_barrier_semaphore()

    @pl.when(me + 1 < n)
    def _():
        pl.semaphore_signal(barrier, inc=1, device_id={"sp": me + 1}, device_id_type=MESH)

    @pl.when(me > 0)
    def _():
        pl.semaphore_signal(barrier, inc=1, device_id={"sp": me - 1}, device_id_type=MESH)

    pl.semaphore_signal(barrier, inc=1, device_id={"tp": across}, device_id_type=MESH)
    pl.semaphore_signal(barrier, inc=1, device_id={"tp": sibling}, device_id_type=MESH)
    pl.semaphore_signal(barrier, inc=1, device_id={"grp": 1 - grp}, device_id_type=MESH)
    pl.semaphore_wait(barrier, jnp.where((me > 0) & (me + 1 < n), 5, 4))
    pltpu.make_async_copy(weights.at[mine_w], weights.at[mine_w], local.at[0]).wait()

    def w_slot(src, m, g):
        return weights.at[pl.ds(pl.multiple_of(src * depth + g * half, half), half),
                          pl.ds(m * cols, cols)]

    def w_hop(src, m, to):
        return pltpu.make_async_remote_copy(
            src_ref=w_slot(src, m, grp), dst_ref=w_slot(src, m, grp),
            send_sem=sent.at[0], recv_sem=w_recv.at[src * 2 + m],
            device_id={"sp": to}, device_id_type=MESH,
        )

    def w_side(src, m, g):
        return pltpu.make_async_remote_copy(
            src_ref=w_slot(src, m, g), dst_ref=w_slot(src, m, g),
            send_sem=sent.at[0], recv_sem=met.at[0],
            device_id={"grp": 1 - grp}, device_id_type=MESH,
        )

    def w_all(count):
        block = weights.at[pl.ds(0, count * half)]
        return pltpu.make_async_remote_copy(
            src_ref=block, dst_ref=block, send_sem=sent.at[1], recv_sem=met.at[0],
            device_id={"grp": 1 - grp}, device_id_type=MESH,
        )

    def z_copy(src, dst, kind, j):
        return pltpu.make_async_remote_copy(
            src_ref=prompt.at[dst, part(kind, j, tp)], dst_ref=rows_in.at[src, part(kind, j, tp)],
            send_sem=sent.at[1], recv_sem=z_recv.at[flag(src, dst, kind, j)],
            device_id={"sp": dst}, device_id_type=MESH,
        )

    def side_copy(src, kind, j, q, to, recv):
        return pltpu.make_async_remote_copy(
            src_ref=rows_in.at[src, part(kind, j, q)], dst_ref=rows_in.at[src, part(kind, j, q)],
            send_sem=sent.at[1], recv_sem=recv.at[flag(src, me, kind, j)],
            device_id={"tp": to}, device_id_type=MESH,
        )

    def both_halves(src, start, size, at):
        rows = rows_in.at[src, pl.ds(pl.multiple_of(start, size), size)]
        return pltpu.make_async_remote_copy(
            src_ref=rows, dst_ref=rows, send_sem=sent.at[1], recv_sem=d_recv.at[at],
            device_id={"tp": sibling}, device_id_type=MESH,
        )

    even = lax.rem(tp, 2) == 0

    def skips(kind, j):
        return kind == "tail" and j >= len(TAIL) - 2

    def take(src, kind, j):
        z_copy(src, me, kind, j).wait_recv()
        side_copy(src, kind, j, tp, across, x_recv).start()
        if skips(kind, j):
            @pl.when(even)
            def _():
                side_copy(src, kind, j, tp, far, d_recv).start()

        side_copy(src, kind, j, tp, sibling, d_recv).start()

    def relay(src, kind, j):
        side_copy(src, kind, j, across, across, x_recv).wait_recv()

        @pl.when(jnp.logical_not(even & skips(kind, j)))
        def _():
            side_copy(src, kind, j, across, sibling, d_recv).start()

    def settle(src, kind, j):
        start, size = span(kind, j)
        both_halves(src, start, size // 2, flag(src, me, kind, j)).wait_recv()

    def send_all(items):
        for dst, kind, j in items:
            z_copy(me, dst, kind, j).start()

    for m in range(2):
        @pl.when(me + 1 < n)
        def _():
            w_hop(me, m, me + 1).start()

        @pl.when(me > 0)
        def _():
            w_hop(me, m, me - 1).start()

    for spot in range(n):
        @pl.when(me == spot)
        def _():
            send_all(right_plan(n, blocks, spot)[0])
            send_all(left_plan(n, blocks, spot)[0])

    own_rows = pltpu.make_async_copy(prompt.at[me], rows_in.at[me], local.at[1])
    small_in = [
        pltpu.make_async_copy(a, b, local.at[at])
        for a, b, at in (
            (query, new_in.at[0], 2), (key_new, new_in.at[1], 2), (value_new, new_in.at[2], 2),
            (lam, lam_in, 3), (gain, gain_in, 4),
        )
    ]
    for copy in [own_rows] + small_in:
        copy.start()

    def weight_event(spot, src):
        for m in range(2):
            if src < spot:
                w_hop(src, m, me).wait_recv()
                if spot + 1 < n:
                    w_hop(src, m, me + 1).start()
            else:
                w_hop(src, m, me).wait_recv()
                if spot > 0:
                    w_hop(src, m, me - 1).start()
            w_side(src, m, grp).start()

    plans = [arrivals(n, blocks, spot) for spot in range(n)]
    aheads = [sum(kind == "big" for kind, _, _ in first) for first, _ in plans]
    orders = [
        [(s, j) for kind, s, j in first if kind == "big"] + [(s, j) for _, s, j in rest]
        for first, rest in plans
    ]
    total = len(orders[0])
    for spot in range(n):
        first = plans[spot][0]
        bigs = []

        @pl.when(me == spot)
        def _():
            lefts = [s for kind, s, _ in first if kind == "w" and s < spot]
            rights = [s for kind, s, _ in first if kind == "w" and s > spot]
            for kind, s, j in first:
                if kind == "w":
                    weight_event(spot, s)
                    if s < spot:
                        lefts.remove(s)
                        if not lefts:
                            send_all(right_plan(n, blocks, spot)[1][:HOLD])
                    else:
                        rights.remove(s)
                        if not rights:
                            send_all(left_plan(n, blocks, spot)[1][:HOLD])
                    continue
                take(s, kind, j)
                if kind == "big":
                    bigs.append((s, j))
                    if len(bigs) > 1:
                        relay(bigs[-2][0], "big", bigs[-2][1])
            if any(kind == "tail" for kind, _, _ in first):
                relay(critical(n, spot), "tail", 0)
            if spot > 0:
                send_all(left_plan(n, blocks, spot)[1][HOLD if spot < n - 1 else 0:])
            if spot < n - 1:
                send_all(right_plan(n, blocks, spot)[1][HOLD if spot > 0 else 0:])

    pltpu.make_async_copy(new_in, new_in, local.at[2]).wait()
    for copy in small_in[3:]:
        copy.wait()

    def mine(which):
        whole = new_in[which].astype(jnp.float32)
        here = lax.broadcasted_iota(jnp.int32, whole.shape, 0) == me
        return jnp.sum(jnp.where(here, whole, 0.0), axis=0, keepdims=True)

    scale = HALF ** (-0.5)
    shape = (2 * heads, cols)
    row = lax.broadcasted_iota(jnp.int32, shape, 0)
    group = lax.broadcasted_iota(jnp.int32, shape, 1) // HALF
    chosen = jnp.where(row < heads, 2 * row, 2 * (row - heads) + 1) == group
    q_mat = jnp.where(chosen, jnp.broadcast_to(mine(0), shape), 0.0)
    fresh = jnp.sum(q_mat * mine(1), axis=1, keepdims=True) * scale
    q_low[...] = q_mat.astype(jnp.bfloat16)
    spread = (heads, heads)
    mix = jnp.sum(
        jnp.where(
            lax.broadcasted_iota(jnp.int32, spread, 0) == lax.broadcasted_iota(jnp.int32, spread, 1),
            jnp.broadcast_to(lam_in[...], spread), 0.0,
        ),
        axis=1, keepdims=True,
    )

    def project_rows(src, start, size):
        both = jnp.dot(
            rows_in[src, pl.ds(start, size), :], weights[...], preferred_element_type=jnp.float32
        ).astype(jnp.bfloat16)
        at = pl.ds(pl.multiple_of(src * piece + start, BIG // 2), size)
        keys[at, :] = both[:, :cols]
        values[at, :] = both[:, cols:]

    def score_rows(src, start, size):
        at = pl.multiple_of(src * piece + start, BIG // 2)
        scores[:, pl.ds(at, size)] = lax.dot_general(
            q_low[...], keys[pl.ds(at, size), :], (((1,), (1,)), ((), ())),
            preferred_element_type=jnp.float32,
        ) * scale

    def compute(src, j):
        start = pl.multiple_of(j * BIG, BIG)
        project_rows(src, start, BIG)
        score_rows(src, start, BIG)

    picks = [by_spot([o[at][0] * blocks + o[at][1] for o in orders]) for at in range(total)]

    def order(k):
        pick = picks[0]
        for at in range(1, total):
            pick = jnp.where(k == at, picks[at], pick)
        return pick // blocks, lax.rem(pick, blocks)

    ahead = by_spot(aheads)

    def step(k, carry):
        src, j = order(k)
        take_big(src, j)
        src, j = order(k - 1)
        relay_big(src, j)

        @pl.when(k == ahead + START)
        def _():
            w_all(n - 1).wait_recv()
            own_rows.wait()

        b = k - ahead - START

        @pl.when((b >= 0) & (b < blocks + ahead))
        def _():
            src, j = order(b - blocks)
            foreign = b >= blocks

            @pl.when(foreign)
            def _():
                settle_big(src, j)

            compute(jnp.where(foreign, src, me), jnp.where(foreign, j, b))

        @pl.when(k - 2 >= ahead)
        def _():
            src, j = order(k - 2)
            settle_big(src, j)
            compute(src, j)

        return carry

    def dyn(j, q):
        quarter = BIG // 4
        return pl.ds(pl.multiple_of(j * BIG + q * quarter, quarter), quarter)

    def z_big(src, dst, j):
        return pltpu.make_async_remote_copy(
            src_ref=prompt.at[dst, dyn(j, tp)], dst_ref=rows_in.at[src, dyn(j, tp)],
            send_sem=sent.at[1], recv_sem=z_recv.at[big_flag(src, dst, j)],
            device_id={"sp": dst}, device_id_type=MESH,
        )

    def side_big(src, j, q, to, recv):
        return pltpu.make_async_remote_copy(
            src_ref=rows_in.at[src, dyn(j, q)], dst_ref=rows_in.at[src, dyn(j, q)],
            send_sem=sent.at[1], recv_sem=recv.at[big_flag(src, me, j)],
            device_id={"tp": to}, device_id_type=MESH,
        )

    def take_big(src, j):
        z_big(src, me, j).wait_recv()
        side_big(src, j, tp, across, x_recv).start()
        side_big(src, j, tp, sibling, d_recv).start()

    def relay_big(src, j):
        side_big(src, j, across, across, x_recv).wait_recv()
        side_big(src, j, across, sibling, d_recv).start()

    def settle_big(src, j):
        both_halves(src, j * BIG, BIG // 2, big_flag(src, me, j)).wait_recv()

    lax.fori_loop(ahead, total, step, 0)

    late_fill = (me == 0) | (me == n - 1)

    @pl.when(late_fill)
    def _():
        take(crit, "tail", 0)

    src, j = order(total - 1)
    relay_big(src, j)

    def last_bigs(k, carry):
        src, j = order(k)

        @pl.when(k < total)
        def _():
            settle_big(src, j)

        @pl.when(k == total - 1)
        def _():
            take(crit, "tail", 1)

            @pl.when(late_fill)
            def _():
                relay(crit, "tail", 0)

        @pl.when(k == total)
        def _():
            take(crit, "tail", 2)
            relay(crit, "tail", 1)
            for piece_ in (3, 4, 5):
                take(crit, "tail", piece_)
            relay(crit, "tail", 2)
            settle(crit, "tail", 0)
            settle(crit, "tail", 1)

        final = k == total
        compute(jnp.where(final, crit, src), jnp.where(final, blocks - 2, j))
        return carry

    lax.fori_loop(total - 2, total + 1, last_bigs, 0)

    relay(crit, "tail", 3)
    settle(crit, "tail", 2)

    @pl.when(jnp.logical_not(even))
    def _():
        for piece_ in (4, 5):
            relay(crit, "tail", piece_)

    project_rows(crit, piece - BIG, BIG // 2)
    score_rows(crit, piece - BIG, BIG // 2)

    @pl.when(even)
    def _():
        for piece_ in (4, 5):
            relay(crit, "tail", piece_)

    for piece_ in (3, 4, 5):
        settle(crit, "tail", piece_)
    rest = BIG // 2
    rest_rows = rows_in[crit, piece - rest:, :]
    at_rest = pl.ds(pl.multiple_of(crit * piece + piece - rest, rest), rest)
    keys[at_rest, :] = jnp.dot(
        rest_rows, weights[:, :cols], preferred_element_type=jnp.float32
    ).astype(jnp.bfloat16)
    score_rows(crit, piece - rest, rest)
    values[at_rest, :] = jnp.dot(
        rest_rows, weights[:, cols:], preferred_element_type=jnp.float32
    ).astype(jnp.bfloat16)

    s = scores[...]
    top = jnp.maximum(jnp.max(s, axis=1, keepdims=True), fresh)
    e = jnp.exp(s - top)
    fresh_e = jnp.exp(fresh - top)
    sums = jnp.sum(e, axis=1, keepdims=True) + fresh_e
    w = e / sums
    fresh_w = fresh_e / sums
    mixed = (w[:heads] - mix * w[heads:]).astype(jnp.bfloat16)
    fresh_mixed = (fresh_w[:heads] - mix * fresh_w[heads:]).astype(jnp.bfloat16).astype(jnp.float32)
    o = jnp.dot(mixed, values[...], preferred_element_type=jnp.float32)
    o = o + fresh_mixed * mine(2)
    for h in range(heads):
        lanes = slice(h * VDIM, (h + 1) * VDIM)
        one = o[h:h + 1, lanes]
        mean = jnp.mean(one * one, axis=1, keepdims=True)
        own[:, lanes] = one * lax.rsqrt(mean + 1e-06) * gain_in[...]

    def row_copy(step_, src):
        return pltpu.make_async_remote_copy(
            src_ref=own, dst_ref=slots.at[src], send_sem=sent.at[2], recv_sem=met.at[1],
            device_id={"sp": lax.rem(me + step_, n)}, device_id_type=MESH,
        )

    for step_ in range(1, n):
        row_copy(step_, me).start()

    def all_sent(block, at):
        pltpu.make_async_remote_copy(
            src_ref=block, dst_ref=block, send_sem=sent.at[at], recv_sem=met.at[1],
            device_id={"sp": lax.rem(me + 1, n)}, device_id_type=MESH,
        ).wait_send()

    all_sent(rows_in.at[pl.ds(0, n - 1)], 1)
    inner = (me > 0) & (me + 1 < n)

    @pl.when(inner)
    def _():
        all_sent(weights.at[pl.ds(0, 2 * n * half)], 0)

    @pl.when(jnp.logical_not(inner))
    def _():
        all_sent(weights.at[pl.ds(0, n * half)], 0)

    others = slots.at[pl.ds(0, n - 1)]
    pltpu.make_async_remote_copy(
        src_ref=others, dst_ref=others, send_sem=sent.at[2], recv_sem=met.at[1],
        device_id={"sp": lax.rem(me + 1, n)}, device_id_type=MESH,
    ).wait_recv()
    mine_row = own[...]
    for src in range(n):
        read[src:src + 1, :] = jnp.where(me == src, mine_row, slots[src]).astype(jnp.bfloat16)
    all_sent(others, 2)


def gather_project(n, prompt, w_key, w_value, query, key_new, value_new, mix_lambda, head_gain):
    count, piece, width = prompt.shape
    depth, cols = w_key.shape
    heads = mix_lambda.shape[0]
    dma = pltpu.SemaphoreType.DMA
    steps = (n - 1) * (piece // BIG) + len(TAIL) - 2
    out = pltpu.VMEM((n * piece, cols), jnp.bfloat16)
    vmem = pl.BlockSpec(memory_space=pltpu.VMEM)
    hbm = pl.BlockSpec(memory_space=pltpu.HBM)
    f32, bf16 = jnp.float32, jnp.bfloat16
    return pl.pallas_call(
        functools.partial(gather_kernel, (n, piece)),
        out_shape=(out, out, pltpu.VMEM((n, cols), bf16)),
        in_specs=[hbm] * 8,
        out_specs=(vmem, vmem, vmem),
        scratch_shapes=[
            pltpu.VMEM((n, piece, width), bf16),
            pltpu.VMEM((n * depth, 2 * cols), bf16),
            pltpu.VMEM((2 * heads, n * piece), f32),
            pltpu.VMEM((2 * heads, cols), bf16),
            pltpu.VMEM((1, cols), f32),
            pltpu.VMEM((n, 1, cols), f32),
            pltpu.VMEM((3, *query.shape), bf16),
            pltpu.VMEM((1, heads), f32),
            pltpu.VMEM((1, VDIM), f32),
        ]
        + [dma((steps,))] * 3
        + [dma((2 * n,)), dma((3,)), dma((2,)), dma((5,))],
        compiler_params=pltpu.CompilerParams(
            collective_id=0, has_side_effects=True,
            vmem_limit_bytes=2**26 - 2**18 - 4 * n * piece * cols,
        ),
    )(
        prompt, w_key, w_value, query, key_new, value_new,
        mix_lambda[None, :], head_gain[None, :],
    )


def write_kernel(cuts, *refs):
    ins, outs, sem = refs[:3], refs[3:6], refs[6]
    copies = []
    for i in range(2):
        size = ins[i].shape[0] // cuts
        for c in range(cuts):
            at = pl.ds(c * size, size)
            copies.append((ins[i].at[at], outs[i].at[at]))
    copies.append((ins[2], outs[2]))
    copies = [pltpu.make_async_copy(a, b, sem.at[i]) for i, (a, b) in enumerate(copies)]
    for copy in copies:
        copy.start()
    for copy in copies:
        copy.wait()


def write_out(keys, values, read):
    cuts = 4
    hbm = pl.BlockSpec(memory_space=pltpu.HBM)
    vmem = pl.BlockSpec(memory_space=pltpu.VMEM)
    return pl.pallas_call(
        functools.partial(write_kernel, cuts),
        out_shape=tuple(jax.ShapeDtypeStruct(a.shape, a.dtype) for a in (keys, values, read)),
        in_specs=[vmem] * 3,
        out_specs=(hbm, hbm, hbm),
        scratch_shapes=[pltpu.SemaphoreType.DMA((2 * cuts + 1,))],
        compiler_params=pltpu.CompilerParams(vmem_limit_bytes=2**20),
    )(keys, values, read)


def fast_body(prompt, w_key, w_value, query_new, key_new, value_new, mix_lambda, head_gain):
    count, piece, width = prompt.shape
    n = lax.axis_size("sp")
    keys, values, read = write_out(
        *gather_project(
            n, prompt, w_key, w_value, query_new, key_new, value_new, mix_lambda, head_gain
        )
    )
    cols = keys.shape[-1]
    return (keys.reshape(1, n, piece, cols), values.reshape(1, n, piece, cols), read)


def choose(mesh):
    def run(prompt, *rest):
        sizes = dict(mesh.shape)
        count, piece, width = prompt.shape
        rows = rest[0].shape[0]
        fits = (
            sizes["grp"] == 2
            and sizes["tp"] == 4
            and sizes["sp"] == count
            and count == 4
            and piece % BIG == 0
            and piece >= 6 * BIG
            and rows % 32 == 0
            and count * piece * width * 2 <= 2**25
        )
        return (fast_body if fits else body)(prompt, *rest)

    return run


def solution(mesh):
    placed = (
        P("grp", "sp", None),
        P("sp", "tp"),
        P("sp", "tp"),
        P("grp", "tp"),
        P("grp", "tp"),
        P("grp", "tp"),
        P("tp"),
        P(),
    )
    return jax.shard_map(
        choose(mesh),
        mesh=mesh,
        in_specs=placed,
        out_specs=(
            P(("grp", "sp"), None, None, "tp"),
            P(("grp", "sp"), None, None, "tp"),
            P("grp", "tp"),
        ),
        check_vma=False,
    )
```
